32 devices in a mesh: grp: 2 (over y), tp: 4 (over z), dp: 4 (over x, core).
Axes of the slice: x: 2, y: 2, z: 4, core: 2. Of those that a mesh axis runs over, the one named last changes fastest.
Arguments:
- tokens: bfloat16 [64, 4096], P(('grp', 'tp'), 'dp'), parts along dimension 0, may hold values from -50 to 50
- norm_gain: float32 [2, 4096], P(None, 'dp'), may hold values from 0.1 to 1.9
- query_weight: bfloat16 [2, 4096, 4096], P(None, 'dp', 'tp'), may hold values from -0.09375 to 0.09375
- key_weight: bfloat16 [2, 4096, 4096], P(None, 'dp', 'tp'), may hold values from -0.09375 to 0.09375
- value_weight: bfloat16 [2, 4096, 4096], P(None, 'dp', 'tp'), may hold values from -0.09375 to 0.09375
- outgate_weight: bfloat16 [2, 4096, 4096], P(None, 'dp', 'tp'), may hold values from -0.09375 to 0.09375
- input_gate_weight: bfloat16 [2, 4096, 64], P(None, 'dp', 'tp'), may hold values from -0.09375 to 0.09375
- forget_gate_weight: bfloat16 [2, 4096, 64], P(None, 'dp', 'tp'), may hold values from -0.09375 to 0.09375
- forget_bias: float32 [2, 64], P(None, 'tp'), may hold values from -2 to 5
- out_weight: bfloat16 [2, 4096, 4096], P(None, 'tp', 'dp'), may hold values from -0.09375 to 0.09375
- memory_state: float32 [2, 64, 64, 4096], P(None, ('grp', 'dp'), 'tp'), parts along dimension 1, may hold values from -0.9 to 0.9
- normalizer_state: float32 [2, 64, 4096], P(None, ('grp', 'dp'), 'tp'), parts along dimension 1, may hold values from -0.9 to 0.9
- maximum_state: float32 [2, 64, 64], P(None, ('grp', 'dp'), 'tp'), parts along dimension 1, may hold values from -1 to 1
Outputs:
- next_tokens: bfloat16 [64, 4096], P(('grp', 'tp'), 'dp'), parts along dimension 0
- next_memory: float32 [2, 64, 64, 4096], P(None, ('grp', 'dp'), 'tp'), parts along dimension 1
- next_normalizer: float32 [2, 64, 4096], P(None, ('grp', 'dp'), 'tp'), parts along dimension 1
- next_maximum: float32 [2, 64, 64], P(None, ('grp', 'dp'), 'tp'), parts along dimension 1
The draws below stay inside these ranges and needn't reach their ends.
There are 2 independent parts, one for each index of `grp`. The reference program is written for one: setup_inputs(seed, part) draws one part's arguments, and reference() takes and returns one part's arrays. A program takes and returns all parts, laid end to end along the dimension named above; an argument that names none is the same for every part. Nothing has to cross between parts.
All inputs are finite; a program needn't handle non-finite values.
Results may differ from the reference program's by a relative error of at most 0.0074.
Values may be sent and summed in bfloat16 or wider, within the bound.
No kernel may reach another device: no remote copies, remote signals or barrier semaphores. Data moves between devices by JAX's collectives and lax.ppermute only.
A program may use at most 128 MiB of HBM per device.

```python
import math
import jax
import jax.numpy as jnp
from jax import lax

D = 4096
HEADS = 64
HEAD = 64
LAYERS = 2
BATCH = 32


def draw_tokens(key, part):
    key_entries = jax.random.fold_in(key, 11)
    key_rows = jax.random.fold_in(key, 12)
    columns = jnp.arange(D, dtype=jnp.float32) / (D - 1) - 0.5
    row_scale = jnp.exp(jax.random.uniform(key_rows, (BATCH, 1), jnp.float32, -1.15, 1.15))
    entries = jnp.clip(jax.random.normal(key_entries, (BATCH, D), jnp.float32), -5.0, 5.0)
    column_ramp = jnp.exp(math.log(10.0) * columns)
    return (entries * row_scale * column_ramp[None, :]).astype(jnp.bfloat16)


def levels(rng, extent, pieces, least, largest):
    def one(position, shards_of):
        steps = jax.random.uniform(jax.random.fold_in(jax.random.fold_in(rng, 6), position), (shards_of,), jnp.float32, least / len(pieces), largest / len(pieces))
        return jnp.repeat(jnp.exp(steps), extent[position] // shards_of).reshape((-1,) + (1,) * (len(extent) - position - 1))

    level = one(*pieces[0])
    for cut in pieces[1:]:
        level = level * one(*cut)
    return level


def scatter_about(key, dims, width, bound, cuts=(), kind=jnp.bfloat16):
    drawn = width * jax.random.normal(key, dims, jnp.float32)
    if cuts:
        drawn = drawn * levels(key, dims, cuts, -0.22, 0.18)
    return jnp.clip(drawn, -bound, bound).astype(kind)


def setup_inputs(seed: int = 0, part: int = 0) -> dict:
    streams_of = jax.random.split(jax.random.key(seed), 14)
    own_keys = jax.random.split(jax.random.fold_in(streams_of[13], part), 14)
    return {
        "tokens": draw_tokens(jax.random.fold_in(jax.random.fold_in(streams_of[13], part), 71), part),
        "norm_gain": jnp.clip(1.0 + 0.18 * jax.random.normal(streams_of[1], (LAYERS, D), jnp.float32), 0.1, 1.9),
        "query_weight": scatter_about(streams_of[2], (LAYERS, D, HEADS * HEAD), D ** -0.5, 0.09375, ((1, 4), (2, 4))),
        "key_weight": scatter_about(streams_of[3], (LAYERS, D, HEADS * HEAD), D ** -0.5, 0.09375, ((1, 4), (2, 4))),
        "value_weight": scatter_about(streams_of[4], (LAYERS, D, HEADS * HEAD), D ** -0.5, 0.09375, ((1, 4), (2, 4))),
        "outgate_weight": scatter_about(streams_of[5], (LAYERS, D, HEADS * HEAD), D ** -0.5, 0.09375, ((1, 4), (2, 4))),
        "input_gate_weight": scatter_about(streams_of[6], (LAYERS, D, HEADS), D ** -0.5, 0.09375, ((1, 4), (2, 4))),
        "forget_gate_weight": scatter_about(streams_of[7], (LAYERS, D, HEADS), D ** -0.5, 0.09375, ((1, 4), (2, 4))),
        "forget_bias": jnp.clip(-2.0 + 7.0 * jax.random.uniform(streams_of[8], (LAYERS, HEADS), jnp.float32) ** levels(streams_of[8], (LAYERS, HEADS), ((1, 4),), -0.2, 0.2), -2.0, 5.0),
        "out_weight": scatter_about(streams_of[9], (LAYERS, HEADS * HEAD, D), (HEADS * HEAD) ** -0.5, 0.09375, ((1, 4), (2, 4))),
        "memory_state": scatter_about(own_keys[10], (LAYERS, BATCH, HEADS, HEAD * HEAD), 0.15, 0.9, ((1, 4), (2, 4)), jnp.float32),
        "normalizer_state": scatter_about(own_keys[11], (LAYERS, BATCH, HEADS * HEAD), 0.15, 0.9, ((1, 4), (2, 4)), jnp.float32),
        "maximum_state": jnp.clip(jax.random.uniform(own_keys[12], (LAYERS, BATCH, HEADS), jnp.float32, -1.0, 1.0) * levels(own_keys[12], (LAYERS, BATCH, HEADS), ((1, 4), (2, 4)), -0.4, 0.0), -1.0, 1.0),
    }


EPS = 1e-06

def reference(tokens, norm_gain, query_weight, key_weight, value_weight, outgate_weight, input_gate_weight, forget_gate_weight, forget_bias, out_weight, memory_state, normalizer_state, maximum_state):
    current = tokens
    memories = []
    normalizers = []
    maxima = []
    batch_rows = tokens.shape[0]
    shape = (batch_rows, HEADS, HEAD)
    for layer_idx in range(LAYERS):
        x_float = current.astype(jnp.float32)
        squares = lax.optimization_barrier(jnp.sum(x_float * x_float, axis=1))
        inv_rms = lax.rsqrt(squares / D + EPS)[:, None]
        scaled = (x_float * norm_gain[layer_idx][None, :]).astype(jnp.bfloat16)

        def project(weight):
            return inv_rms * jnp.dot(scaled, weight, preferred_element_type=jnp.float32)

        def rounded(weight):
            stored = lax.optimization_barrier(project(weight).astype(jnp.bfloat16))
            return stored.astype(jnp.float32).reshape(shape)
        query_vec = rounded(query_weight[layer_idx])
        key_vec = rounded(key_weight[layer_idx]) * HEAD ** (-0.5)
        value_vec = rounded(value_weight[layer_idx])
        gate_vec = rounded(outgate_weight[layer_idx])
        input_pre = project(input_gate_weight[layer_idx])
        forget_pre = project(forget_gate_weight[layer_idx]) + forget_bias[layer_idx][None, :]
        log_forget = jax.nn.log_sigmoid(forget_pre)
        old_max = maximum_state[layer_idx]
        new_max = jnp.maximum(log_forget + old_max, input_pre)
        keep_rate = jnp.exp(log_forget + old_max - new_max)
        admit_rate = jnp.exp(input_pre - new_max)
        memory = memory_state[layer_idx].reshape(batch_rows, HEADS, HEAD, HEAD)
        memory = keep_rate[:, :, None, None] * memory + admit_rate[:, :, None, None] * key_vec[:, :, :, None] * value_vec[:, :, None, :]
        normalizer = keep_rate[:, :, None] * normalizer_state[layer_idx].reshape(shape) + admit_rate[:, :, None] * key_vec
        numerator = jnp.einsum('bhd,bhde->bhe', query_vec, memory, precision=lax.Precision.HIGHEST)
        denominator = lax.optimization_barrier(jnp.sum(query_vec * normalizer, axis=2))
        readout = numerator / jnp.maximum(jnp.abs(denominator), jnp.exp(-new_max))[:, :, None]
        mixed = (readout * jax.nn.sigmoid(gate_vec)).astype(jnp.bfloat16).reshape(batch_rows, HEADS * HEAD)
        summed = jnp.dot(mixed, out_weight[layer_idx], preferred_element_type=jnp.float32)
        current = (x_float + summed).astype(jnp.bfloat16)
        memories.append(memory.reshape(batch_rows, HEADS, HEAD * HEAD))
        normalizers.append(normalizer.reshape(batch_rows, HEADS * HEAD))
        maxima.append(new_max)
    return (current, jnp.stack(memories), jnp.stack(normalizers), jnp.stack(maxima))
```

```python
import functools

import jax
import jax.numpy as jnp
from jax import lax
from jax.experimental import pallas as pl
from jax.experimental.pallas import tpu as pltpu
from jax.sharding import PartitionSpec as P


HEAD = 64
LANES = 128
EPS = 1e-06
F32 = jnp.float32
BF16 = jnp.bfloat16
VMEM_LIMIT = 10 * 1024 * 1024
LOAD_FLOPS = 30_000_000


def is_pow2(n):
    return n & (n - 1) == 0


def peer_to(me, step, n):
    return me ^ step if is_pow2(n) else lax.rem(me + step, n)


def peer_from(me, step, n):
    return me ^ step if is_pow2(n) else lax.rem(me + n - step, n)


def exchange(blocks, axis, n):
    out = {}
    for s in reversed(range(1, n)):
        pairs = [(i, i ^ s if is_pow2(n) else (i + s) % n) for i in range(n)]
        out[s] = lax.ppermute(blocks[s - 1], axis, pairs)
    return [out[s] for s in range(1, n)]


def tree_sum(terms):
    terms = list(terms)
    while len(terms) > 1:
        nxt = [a + b for a, b in zip(terms[0::2], terms[1::2])]
        if len(terms) % 2:
            nxt.append(terms[-1])
        terms = nxt
    return terms[0]


def call(body, out_shape, in_specs, out_specs, scratch, flops, aliases=None):
    return pl.pallas_call(
        body,
        grid=(1,),
        out_shape=out_shape,
        in_specs=in_specs,
        out_specs=out_specs,
        scratch_shapes=scratch,
        input_output_aliases=aliases or {},
        compiler_params=pltpu.CompilerParams(vmem_limit_bytes=VMEM_LIMIT),
        cost_estimate=pl.CostEstimate(flops=flops, bytes_accessed=1 << 20, transcendentals=0),
    )


SMEM = pl.BlockSpec(memory_space=pltpu.SMEM)
VMEM = pl.BlockSpec(memory_space=pltpu.VMEM)
ANY = pl.BlockSpec(memory_space=pl.ANY)
HBM = pl.BlockSpec(memory_space=pltpu.HBM)


def layer_block(array, layer, rank=3):
    if array.ndim < rank:
        return VMEM
    rest = array.shape[1:]
    zeros = (0,) * len(rest)
    return pl.BlockSpec((None,) + rest, lambda _: (layer,) + zeros)


def half_width(heads):
    return -(-(2 * heads + 1) // 64) * 64


def project(x, gain, weights, gates, own_ref, send_refs, acc, tail, me_dp, n_dp, arrived=None):
    batch = x.shape[0]
    width = weights[0].shape[1]
    heads = gates[0].shape[0]
    half = half_width(heads)
    scaled = (x * gain).astype(BF16)
    tail[...] = jnp.zeros_like(tail)
    for i in range(2):
        tail[:, i * heads : (i + 1) * heads] = lax.dot_general(
            scaled, gates[i][...], (((1,), (1,)), ((), ())), preferred_element_type=F32
        )
    tail[:, 2 * heads : 2 * heads + 1] = jnp.sum(x * x, axis=1, keepdims=True)
    full = tail[...]
    high = full.astype(BF16).astype(F32)
    acc[:, 4 * width :] = high + pltpu.roll(full - high, half, 1)
    step = min(width, 256)
    for i in range(4):
        if arrived:
            arrived(i)
        for c in range(0, width, step):
            acc[:, i * width + c : i * width + c + step] = jnp.dot(
                scaled, weights[i][:, c : c + step], preferred_element_type=F32
            )
    rows = batch // n_dp
    own_ref[...] = acc[pl.ds(pl.multiple_of(me_dp * rows, rows), rows), :]
    for s in range(1, n_dp):
        to = peer_to(me_dp, s, n_dp)
        send_refs[s - 1][...] = acc[pl.ds(pl.multiple_of(to * rows, rows), rows), :].astype(BF16)


def load_kernel(count, *refs):
    sources, outs, sems = refs[:count], refs[count:-1], refs[-1]
    copies = [
        pltpu.make_async_copy(source if out.shape == source.shape else source.at[0], out, sems.at[i])
        for i, (source, out) in enumerate(zip(sources, outs))
    ]
    for copy in copies:
        copy.start()
    for copy in copies:
        copy.wait()


def in_hbm(array):
    return pltpu.with_memory_space_constraint(array, pltpu.HBM)


def load(flat, stacked):
    sources = [*flat, *stacked]
    shapes = [(w.shape, w.dtype) for w in flat] + [(w.shape[1:], w.dtype) for w in stacked]
    return call(
        functools.partial(load_kernel, len(sources)),
        [jax.ShapeDtypeStruct(shape, dtype) for shape, dtype in shapes],
        [HBM] * len(sources), [VMEM] * len(shapes),
        [pltpu.SemaphoreType.DMA((len(sources),))], LOAD_FLOPS,
    )(*[in_hbm(w) for w in sources])


def first_kernel(n_tp, n_dp, idx, *refs):
    xs, refs = refs[:n_tp], refs[n_tp:]
    gain, refs = refs[0], refs[1:]
    weights, gates, refs = refs[:4], refs[4:6], refs[6:]
    x_out, own, sends = refs[0], refs[1], refs[2 : 2 + n_dp - 1]
    acc, tail, streamed, sems = refs[-4:]
    copies = [
        pltpu.make_async_copy(weights[2 + i].at[0], streamed.at[i], sems.at[i]) for i in range(2)
    ]
    for copy in copies:
        copy.start()
    me_tp, me_dp = idx[0], idx[1]
    rows = xs[0].shape[0]
    for s in range(n_tp):
        at = pl.multiple_of(peer_from(me_tp, s, n_tp) * rows, rows)
        x_out[pl.ds(at, rows), :] = xs[s][...].astype(F32)

    def arrived(i):
        if i >= 2:
            copies[i - 2].wait()

    weights = [*weights[:2], streamed.at[0], streamed.at[1]]
    project(
        x_out[...], gain[0:1, :], weights, gates, own, sends, acc, tail, me_dp, n_dp, arrived
    )


def later_kernel(n_tp, n_dp, layer, idx, x_prev, *refs):
    parts, refs = refs[:n_tp], refs[n_tp:]
    gain, refs = refs[0], refs[1:]
    weights, gates, refs = refs[:4], refs[4:6], refs[6:]
    x_out, own, sends, acc, tail = refs[0], refs[1], refs[2 : 2 + n_dp - 1], refs[-2], refs[-1]
    total = tree_sum(p[...].astype(F32) for p in parts)
    x = (x_prev[...] + total).astype(BF16).astype(F32)
    x_out[...] = x
    project(x, gain[layer : layer + 1, :], weights, gates, own, sends, acc, tail, idx[1], n_dp)


def projection(idx, x_prev, pieces, layer, gain, weights, gates, batch, n_tp, n_dp):
    features, width = weights[0].shape[-2:]
    heads = gates[0].shape[-2]
    total = 4 * width + 2 * half_width(heads)
    rows = batch // n_dp
    out_shape = (
        [jax.ShapeDtypeStruct((batch, features), F32), jax.ShapeDtypeStruct((rows, total), F32)]
        + [jax.ShapeDtypeStruct((rows, total), BF16)] * (n_dp - 1)
    )
    first = x_prev is None
    lead = [idx] if first else [idx, x_prev]
    body = functools.partial(first_kernel, n_tp, n_dp) if first else functools.partial(
        later_kernel, n_tp, n_dp, layer
    )
    in_specs = (
        [SMEM] + [VMEM] * (len(lead) - 1 + len(pieces) + 1)
        + [VMEM if w.ndim == 2 else HBM if first else layer_block(w, layer) for w in (*weights, *gates)]
    )
    scratch = [
        pltpu.VMEM((batch, total), F32),
        pltpu.VMEM((batch, 2 * half_width(heads)), F32),
    ]
    if first:
        scratch += [pltpu.VMEM((2, features, width), BF16), pltpu.SemaphoreType.DMA((2,))]
    out = call(
        body, out_shape, in_specs, [VMEM] * len(out_shape), scratch, 30_000_000
    )(*lead, *pieces, gain, *weights, *gates)
    return out[0], out[1], out[2:]


def column(row, eye):
    return jnp.sum(jnp.where(eye, row, 0.0), axis=1, keepdims=True)


def spread_index(shape, j):
    lane = lax.broadcasted_iota(jnp.int32, shape, 1)
    return jnp.where(lane >= HEAD, 2 * j + 1, 2 * j)


def take_lanes(x, index):
    return jnp.take_along_axis(x, index, axis=1)


def spread_matrix(tile):
    row = lax.broadcasted_iota(jnp.int32, (LANES, 2 * LANES), 0)
    lane = lax.broadcasted_iota(jnp.int32, (LANES, 2 * LANES), 1)
    return jnp.where(row - lane // HEAD == 2 * LANES // HEAD * tile, 1.0, 0.0).astype(BF16)


def swap_matrix(outer, inner):
    size = outer * inner
    to = lax.broadcasted_iota(jnp.int32, (size, size), 0)
    source = lax.broadcasted_iota(jnp.int32, (size, size), 1)
    same = (to // inner == source % outer) & (to % inner == source // outer)
    return jnp.where(same, 1.0, 0.0).astype(BF16)


def pieces_of(x, count):
    out = []
    for _ in range(count - 1):
        high = x.astype(BF16).astype(F32)
        out.append(high)
        x = x - high
    return [*out, x]


def lanes_to_rows(x):
    low = lax.broadcasted_iota(jnp.int32, (x.shape[0], LANES), 1) < HEAD
    out = []
    for c in range(0, x.shape[1], LANES):
        chunk = x[:, c : c + LANES]
        turned = pltpu.roll(chunk, HEAD, 1)
        out += [jnp.where(low, chunk, turned), jnp.where(low, turned, chunk)]
    return jnp.concatenate(out, axis=0)


def readout_kernel(n_dp, width, heads, model, layer, *refs):
    parts, refs = refs[:n_dp], refs[n_dp:]
    bias, old_max, old_norm, memory, refs = *refs[:4], refs[4:]
    mixed_out, keep_out, admit_out, key_out, key_rows, value_rows, max_out = refs
    rows = mixed_out.shape[0]
    half = half_width(heads)
    total = tree_sum(p[...].astype(F32) for p in parts)
    tail = total[:, 4 * width :]
    tail = tail + pltpu.roll(tail, half, 1)
    inv = lax.rsqrt(tail[:, 2 * heads : 2 * heads + 1] / model + EPS)
    stored = [
        (inv * total[:, i * width : (i + 1) * width]).astype(BF16).astype(F32) for i in range(4)
    ]
    query, key = stored[0], stored[1]
    by_head = jnp.concatenate([lanes_to_rows(x) for x in stored], axis=1).astype(BF16)
    by_row = jnp.dot(swap_matrix(rows, heads), by_head, preferred_element_type=F32)
    query_rows = by_row[:, 0:LANES].astype(BF16)
    key_rows[...] = by_row[:, LANES : 2 * LANES].astype(BF16)
    value_row = by_row[:, 2 * LANES : 3 * LANES]
    value_rows[...] = value_row
    past = jnp.zeros((rows * heads, LANES), F32)
    for tile in range(HEAD * HEAD // (2 * LANES)):
        spread = jnp.dot(query_rows, spread_matrix(tile), preferred_element_type=F32)
        for c in range(0, 2 * LANES, LANES):
            at = tile * 2 * LANES + c
            block = memory[:, :, at : at + LANES].reshape(rows * heads, LANES)
            past = past + spread[:, c : c + LANES] * block
    past = past + pltpu.roll(past, HEAD, 1)

    input_pre = inv * tail[:, 0:heads]
    forget_pre = inv * tail[:, heads : 2 * heads] + bias[layer : layer + 1, :]
    log_forget = jnp.minimum(forget_pre, 0.0) - jnp.log1p(jnp.exp(-jnp.abs(forget_pre)))
    aged = log_forget + old_max[...]
    new_max = jnp.maximum(aged, input_pre)
    keep = jnp.exp(aged - new_max)
    admit = jnp.exp(input_pre - new_max) * HEAD**-0.5
    group = lax.broadcasted_iota(jnp.int32, (width, LANES), 0)
    lane = lax.broadcasted_iota(jnp.int32, (width, LANES), 1)
    head_of = jnp.where(group // HEAD == lane, 1.0, 0.0).astype(BF16)
    products = pieces_of(query * key, 2) + pieces_of(query * old_norm[...], 3)
    products.append(jnp.zeros_like(query))
    sums = jnp.dot(
        jnp.concatenate(products, axis=0).astype(BF16), head_of, preferred_element_type=F32
    )[:, 0:heads]
    query_key = sums[0:rows] + sums[rows : 2 * rows]
    query_norm = sums[2 * rows : 3 * rows] + (sums[3 * rows : 4 * rows] + sums[4 * rows : 5 * rows])
    gained = admit * query_key
    denominator = jnp.maximum(jnp.abs(keep * query_norm + gained), jnp.exp(-new_max))
    max_out[...] = new_max
    keep_out[...] = jnp.zeros_like(keep_out)
    admit_out[...] = jnp.zeros_like(admit_out)
    keep_out[:, 0:heads] = keep
    admit_out[:, 0:heads] = admit
    key_out[...] = key

    eye = lax.broadcasted_iota(jnp.int32, (heads, heads), 0) == lax.broadcasted_iota(
        jnp.int32, (heads, heads), 1
    )
    read = []
    for s in range(rows):
        at = slice(s * heads, (s + 1) * heads)
        numerator = (
            column(keep[s : s + 1], eye) * past[at] + column(gained[s : s + 1], eye) * value_row[at]
        )
        read.append(numerator / column(denominator[s : s + 1], eye))
    gate = by_row[:, 3 * LANES :]
    gated = (jnp.concatenate(read, axis=0) * jax.nn.sigmoid(gate)).astype(BF16)
    back = jnp.dot(swap_matrix(heads, rows), gated, preferred_element_type=F32)
    low = lax.broadcasted_iota(jnp.int32, (rows, LANES), 1) < HEAD
    for h in range(0, heads, 2):
        even, odd = back[h * rows : (h + 1) * rows], back[(h + 1) * rows : (h + 2) * rows]
        mixed_out[:, h * HEAD : (h + 2) * HEAD] = jnp.where(low, even, odd).astype(BF16)


def readout(parts, bias, old_max, old_norm, memory, layer, model):
    rows, heads = old_max.shape[-2:]
    width = heads * HEAD
    out_shape = [
        jax.ShapeDtypeStruct((rows, width), BF16),
        jax.ShapeDtypeStruct((rows, LANES), F32),
        jax.ShapeDtypeStruct((rows, LANES), F32),
        jax.ShapeDtypeStruct((rows, width), F32),
        jax.ShapeDtypeStruct((rows * heads, LANES), BF16),
        jax.ShapeDtypeStruct((rows * heads, LANES), F32),
        jax.ShapeDtypeStruct((rows, heads), F32),
    ]
    in_specs = [VMEM] * (len(parts) + 1) + [
        layer_block(old_max, layer), layer_block(old_norm, layer), layer_block(memory, layer, 4)
    ]
    return call(
        functools.partial(readout_kernel, len(parts), width, heads, model, layer),
        out_shape, in_specs, [VMEM] * len(out_shape), [], 20_000_000,
    )(*parts, bias, old_max, old_norm, memory)


def update_kernel(layer, *refs):
    keep_in, admit_in, key_in, key_rows, value_rows, max_in, memory, old_norm = refs[:8]
    earlier = refs[8 : 8 + (3 if layer else 0)]
    memory_out, norm_out, max_out, stage, keep_rows, gain_rows, sems = refs[8 + len(earlier) :]
    rows, heads, size = memory.shape
    eye = lax.broadcasted_iota(jnp.int32, (heads, heads), 0) == lax.broadcasted_iota(
        jnp.int32, (heads, heads), 1
    )
    for s in range(rows):
        at = slice(s * heads, (s + 1) * heads)
        keep_rows[at] = jnp.broadcast_to(column(keep_in[s : s + 1, 0:heads], eye), (heads, LANES))
        gain_rows[at] = column(admit_in[s : s + 1, 0:heads], eye) * value_rows[at]
    copies = []
    tiles = size // (2 * LANES)
    group = tiles // sems.shape[0]
    for tile in range(tiles):
        spread = jnp.dot(key_rows[...], spread_matrix(tile), preferred_element_type=F32)
        for c in range(0, 2 * LANES, LANES):
            cols = slice(tile * 2 * LANES + c, tile * 2 * LANES + c + LANES)
            block = memory[:, :, cols].reshape(rows * heads, LANES)
            fresh = keep_rows[...] * block + spread[:, c : c + LANES] * gain_rows[...]
            stage[:, :, cols] = fresh.reshape(rows, heads, LANES)
        if tile % group == group - 1:
            cols = pl.ds((tile - group + 1) * 2 * LANES, group * 2 * LANES)
            copy = pltpu.make_async_copy(
                stage.at[:, :, cols], memory_out.at[layer, :, :, cols], sems.at[tile // group]
            )
            copy.start()
            copies.append(copy)
    for j in range(heads * HEAD // LANES):
        cols = slice(j * LANES, (j + 1) * LANES)
        index = spread_index((rows, LANES), j)
        norm_out[layer, :, cols] = (
            take_lanes(keep_in[...], index) * old_norm[:, cols]
            + take_lanes(admit_in[...], index) * key_in[:, cols]
        )
    max_out[layer] = max_in[...]
    if layer:
        norm_out[0:layer] = earlier[1][0:layer]
        max_out[0:layer] = earlier[2][0:layer]
    for copy in copies:
        copy.wait()


def update(read, memory, old_norm, layer, layers, earlier):
    rows, heads, size = memory.shape[-3:]
    out_shape = [
        jax.ShapeDtypeStruct((layers, rows, heads, size), F32),
        jax.ShapeDtypeStruct((layers, rows, heads * HEAD), F32),
        jax.ShapeDtypeStruct((layers, rows, heads), F32),
    ]
    _, keep, admit, key, key_rows, value_rows, new_max = read
    in_specs = [VMEM] * 6 + [layer_block(memory, layer, 4), layer_block(old_norm, layer)]
    in_specs += [ANY, VMEM, VMEM] if layer else []
    return call(
        functools.partial(update_kernel, layer),
        out_shape, in_specs, [ANY, VMEM, VMEM],
        [
            pltpu.VMEM((rows, heads, size), F32),
            pltpu.VMEM((rows * heads, LANES), F32),
            pltpu.VMEM((rows * heads, LANES), F32),
            pltpu.SemaphoreType.DMA((4,)),
        ],
        20_000_000, {8: 0} if layer else None,
    )(keep, admit, key, key_rows, value_rows, new_max, memory, old_norm, *(earlier or ()))


def gather_rows(refs, me, n, scratch):
    rows = refs[0].shape[0]
    for s in range(n):
        at = pl.multiple_of(peer_from(me, s, n) * rows, rows)
        scratch[pl.ds(at, rows), :] = refs[s][...].astype(F32)
    return scratch[...].astype(BF16)


def out_kernel(n_dp, idx, *refs):
    parts, weight, out, rows = refs[:n_dp], refs[n_dp], refs[n_dp + 1], refs[n_dp + 2]
    mixed = gather_rows(parts, idx[1], n_dp, rows)
    step = min(weight.shape[1], 256)
    for c in range(0, weight.shape[1], step):
        out[:, c : c + step] = jnp.dot(
            mixed, weight[:, c : c + step], preferred_element_type=F32
        ).astype(BF16)


def last_out_kernel(n_dp, n_tp, idx, *refs):
    parts, weight, refs = refs[:n_dp], refs[n_dp], refs[n_dp + 1 :]
    own, sends, rows, acc = refs[0], refs[1 : n_tp], refs[-2], refs[-1]
    mixed = gather_rows(parts, idx[1], n_dp, rows)
    step = min(weight.shape[1], 256)
    for c in range(0, weight.shape[1], step):
        acc[:, c : c + step] = jnp.dot(mixed, weight[:, c : c + step], preferred_element_type=F32)
    count = own.shape[0]
    own[...] = acc[pl.ds(pl.multiple_of(idx[0] * count, count), count), :]
    for s in range(1, n_tp):
        at = pl.multiple_of(peer_to(idx[0], s, n_tp) * count, count)
        sends[s - 1][...] = acc[pl.ds(at, count), :].astype(BF16)


def out_projection(idx, parts, weight, layer, n_tp, last):
    n_dp = len(parts)
    rows, width = parts[0].shape
    batch, columns = rows * n_dp, weight.shape[-1]
    in_specs = [SMEM] + [VMEM] * n_dp + [layer_block(weight, layer)]
    scratch = [pltpu.VMEM((batch, width), F32)]
    if last:
        count = batch // n_tp
        out_shape = [jax.ShapeDtypeStruct((count, columns), F32)]
        out_shape += [jax.ShapeDtypeStruct((count, columns), BF16)] * (n_tp - 1)
        body = functools.partial(last_out_kernel, n_dp, n_tp)
        scratch.append(pltpu.VMEM((batch, columns), F32))
    else:
        out_shape = [jax.ShapeDtypeStruct((batch, columns), BF16)]
        body = functools.partial(out_kernel, n_dp)
    return call(
        body, out_shape, in_specs, [VMEM] * len(out_shape), scratch, 15_000_000
    )(idx, *parts, weight)


def final_kernel(idx, x, *refs):
    parts, out = refs[:-1], refs[-1]
    count = out.shape[0]
    base = x[pl.ds(pl.multiple_of(idx[0] * count, count), count), :]
    out[...] = (base + tree_sum(p[...].astype(F32) for p in parts)).astype(BF16)


def final_add(idx, x, parts):
    return call(
        final_kernel, jax.ShapeDtypeStruct(parts[0].shape, BF16),
        [SMEM] + [VMEM] * (len(parts) + 1), VMEM, [], 1_000_000,
    )(idx, x, *parts)


def plain_cell(parts, bias, old_max, old_norm, memory, layer, model):
    rows, heads = old_max.shape[1:]
    width, half = heads * HEAD, half_width(heads)
    total = tree_sum(p.astype(F32) for p in parts)
    tail = total[:, 4 * width : 4 * width + half] + total[:, 4 * width + half :]
    inv = lax.rsqrt(tail[:, 2 * heads : 2 * heads + 1] / model + EPS)
    stored = lax.optimization_barrier((inv * total[:, : 4 * width]).astype(BF16)).astype(F32)
    query, key, value, gate = (
        stored[:, i * width : (i + 1) * width].reshape(rows, heads, HEAD) for i in range(4)
    )
    key = key * HEAD**-0.5
    input_pre = inv * tail[:, 0:heads]
    forget_pre = inv * tail[:, heads : 2 * heads] + bias[layer][None, :]
    aged = jax.nn.log_sigmoid(forget_pre) + old_max[layer]
    new_max = jnp.maximum(aged, input_pre)
    keep, admit = jnp.exp(aged - new_max), jnp.exp(input_pre - new_max)
    state = memory[layer].reshape(rows, heads, HEAD, HEAD)
    state = (
        keep[:, :, None, None] * state
        + admit[:, :, None, None] * key[:, :, :, None] * value[:, :, None, :]
    )
    norm = keep[:, :, None] * old_norm[layer].reshape(rows, heads, HEAD) + admit[:, :, None] * key
    top = jnp.einsum("bhd,bhde->bhe", query, state, precision=lax.Precision.HIGHEST)
    bottom = jnp.maximum(jnp.abs(jnp.sum(query * norm, axis=2)), jnp.exp(-new_max))
    mixed = (top / bottom[:, :, None] * jax.nn.sigmoid(gate)).astype(BF16).reshape(rows, width)
    return mixed, state.reshape(rows, heads, -1), norm.reshape(rows, width), new_max


def fills_tiles(memory):
    return memory.shape[1] % 8 == 0 and memory.shape[2] % 8 == 0


def per_device(
    n_tp, n_dp, tokens, norm_gain, query_weight, key_weight, value_weight, outgate_weight,
    input_gate_weight, forget_gate_weight, forget_bias, out_weight, memory_state,
    normalizer_state, maximum_state,
):
    layers = memory_state.shape[0]
    batch = tokens.shape[0] * n_tp
    model = query_weight.shape[1] * n_dp
    idx = jnp.stack([lax.axis_index("tp"), lax.axis_index("dp")]).astype(jnp.int32)
    weights = (query_weight, key_weight, value_weight, outgate_weight)
    gates = tuple(jnp.swapaxes(g, 1, 2) for g in (input_gate_weight, forget_gate_weight))
    x_all = None
    pieces = exchange([tokens] * (n_tp - 1), "tp", n_tp)
    own, gain, *loaded = load((tokens, norm_gain), (*gates, *weights[:2]))
    loaded += [in_hbm(w) for w in weights[2:]]
    pieces = [own] + pieces
    tiled = fills_tiles(memory_state)
    states, plain = None, []
    for layer in range(layers):
        gain, used = (gain, loaded) if layer == 0 else (norm_gain, (*gates, *weights))
        x_all, own, sends = projection(
            idx, x_all, pieces, layer, gain, used[2:], used[:2], batch, n_tp, n_dp
        )
        parts = [own] + exchange(sends, "dp", n_dp)
        bias, ahead = forget_bias, (maximum_state, normalizer_state, memory_state, out_weight)
        if tiled and layer == 0:
            bias, *ahead = load((forget_bias,), ahead)
        old_max, old_norm, memory, project_out = ahead
        if tiled:
            read = readout(parts, bias, old_max, old_norm, memory, layer, model)
            mixed = read[0]
        else:
            mixed, *rest = plain_cell(parts, bias, old_max, old_norm, memory, layer, model)
            plain.append(rest)
        mixes = [mixed] + exchange([mixed] * (n_dp - 1), "dp", n_dp)
        if tiled:
            states = update(read, memory, old_norm, layer, layers, states)
        last = layer == layers - 1
        part = out_projection(idx, mixes, project_out, layer, n_tp, last)
        sends = part[1:] if last else [part[0]] * (n_tp - 1)
        pieces = [part[0]] + exchange(sends, "tp", n_tp)
    next_tokens = final_add(idx, x_all, pieces)
    if plain:
        states = [jnp.stack(column) for column in zip(*plain)]
    return (next_tokens, *states)


def solution(mesh):
    sizes = dict(mesh.shape)
    in_specs = (
        P(("grp", "tp"), "dp"),
        P(None, "dp"),
        P(None, "dp", "tp"),
        P(None, "dp", "tp"),
        P(None, "dp", "tp"),
        P(None, "dp", "tp"),
        P(None, "dp", "tp"),
        P(None, "dp", "tp"),
        P(None, "tp"),
        P(None, "tp", "dp"),
        P(None, ("grp", "dp"), "tp", None),
        P(None, ("grp", "dp"), "tp"),
        P(None, ("grp", "dp"), "tp"),
    )
    out_specs = (
        P(("grp", "tp"), "dp"),
        P(None, ("grp", "dp"), "tp", None),
        P(None, ("grp", "dp"), "tp"),
        P(None, ("grp", "dp"), "tp"),
    )
    n_tp, n_dp = sizes["tp"], sizes["dp"]

    def whole(*args):
        return per_device(n_tp, n_dp, *args)

    def step(*args):
        sharded = jax.shard_map(
            whole, mesh=mesh, in_specs=in_specs, out_specs=out_specs, check_vma=False
        )
        return sharded(*args)

    return step
```

```python
import functools
import math

import jax
import jax.numpy as jnp
from jax import lax
from jax.experimental import pallas as pl
from jax.experimental.pallas import tpu as pltpu
from jax.sharding import PartitionSpec as P


HEAD = 64
LANES = 128
EPS = 1e-06
F32 = jnp.float32
BF16 = jnp.bfloat16
VMEM_LIMIT = 10 * 1024 * 1024
LOAD_FLOPS = 30_000_000


def is_pow2(n):
    return n & (n - 1) == 0


def peer_to(me, step, n):
    return me ^ step if is_pow2(n) else lax.rem(me + step, n)


def peer_from(me, step, n):
    return me ^ step if is_pow2(n) else lax.rem(me + n - step, n)


def exchange(blocks, axis, n):
    out = {}
    for s in reversed(range(1, n)):
        pairs = [(i, i ^ s if is_pow2(n) else (i + s) % n) for i in range(n)]
        out[s] = lax.ppermute(blocks[s - 1], axis, pairs)
    return [out[s] for s in range(1, n)]


def tree_sum(terms):
    terms = list(terms)
    while len(terms) > 1:
        nxt = [a + b for a, b in zip(terms[0::2], terms[1::2])]
        if len(terms) % 2:
            nxt.append(terms[-1])
        terms = nxt
    return terms[0]


def call(body, out_shape, in_specs, out_specs, scratch, flops, aliases=None):
    return pl.pallas_call(
        body,
        grid=(1,),
        out_shape=out_shape,
        in_specs=in_specs,
        out_specs=out_specs,
        scratch_shapes=scratch,
        input_output_aliases=aliases or {},
        compiler_params=pltpu.CompilerParams(vmem_limit_bytes=VMEM_LIMIT),
        cost_estimate=pl.CostEstimate(flops=flops, bytes_accessed=1 << 20, transcendentals=0),
    )


SMEM = pl.BlockSpec(memory_space=pltpu.SMEM)
VMEM = pl.BlockSpec(memory_space=pltpu.VMEM)
ANY = pl.BlockSpec(memory_space=pl.ANY)
HBM = pl.BlockSpec(memory_space=pltpu.HBM)


def half_width(heads):
    return -(-(2 * heads + 1) // 64) * 64


def project(x, gain, weights, gates, own_ref, send_refs, acc, tail, me_dp, n_dp, arrived=None):
    batch = x.shape[0]
    width = weights[0].shape[1]
    heads = gates[0].shape[0]
    half = half_width(heads)
    scaled = (x * gain).astype(BF16)
    tail[...] = jnp.zeros_like(tail)
    for i in range(2):
        tail[:, i * heads : (i + 1) * heads] = lax.dot_general(
            scaled, gates[i][...], (((1,), (1,)), ((), ())), preferred_element_type=F32
        )
    tail[:, 2 * heads : 2 * heads + 1] = jnp.sum(x * x, axis=1, keepdims=True)
    full = tail[...]
    high = full.astype(BF16).astype(F32)
    acc[:, 4 * width :] = high + pltpu.roll(full - high, half, 1)
    step = min(width, 256)
    for i in range(4):
        for c in range(0, width, step):
            if arrived:
                arrived(i, c)
            acc[:, i * width + c : i * width + c + step] = jnp.dot(
                scaled, weights[i][:, c : c + step], preferred_element_type=F32
            )
    rows = batch // n_dp
    own_ref[...] = acc[pl.ds(pl.multiple_of(me_dp * rows, rows), rows), :]
    for s in range(1, n_dp):
        to = peer_to(me_dp, s, n_dp)
        send_refs[s - 1][...] = acc[pl.ds(pl.multiple_of(to * rows, rows), rows), :].astype(BF16)


def cut(extent, unit):
    count = next((n for n in (4, 2) if extent % (n * unit) == 0), 1)
    return [slice(i * extent // count, (i + 1) * extent // count) for i in range(count)]


def load_plan(shape, dtype):
    large = math.prod(shape) * jnp.dtype(dtype).itemsize >= 1 << 19
    return cut(shape[0], 1 if len(shape) > 2 else 16) if large else [slice(0, shape[0])]


def load_kernel(layers, *refs):
    count = len(layers)
    sources, outs, sems = refs[:count], refs[count:-1], refs[-1]
    copies = []
    for source, out, layer in zip(sources, outs, layers):
        whole = source if layer is None else source.at[layer]
        for rows in load_plan(out.shape, out.dtype):
            sem = sems.at[len(copies)]
            copies.append(pltpu.make_async_copy(whole.at[rows], out.at[rows], sem))
            copies[-1].start()
    for copy in copies:
        copy.wait()


def in_hbm(array):
    return pltpu.with_memory_space_constraint(array, pltpu.HBM)


def load(flat, stacked, layer):
    layers = [None] * len(flat) + [layer] * len(stacked)
    shapes = [(w.shape, w.dtype) for w in flat] + [(w.shape[1:], w.dtype) for w in stacked]
    count = sum(len(load_plan(*entry)) for entry in shapes)
    return call(
        functools.partial(load_kernel, layers),
        [jax.ShapeDtypeStruct(shape, dtype) for shape, dtype in shapes],
        [HBM] * len(layers), [VMEM] * len(shapes),
        [pltpu.SemaphoreType.DMA((count,))], LOAD_FLOPS,
    )(*[in_hbm(w) for w in (*flat, *stacked)])


def first_kernel(n_tp, n_dp, idx, *refs):
    xs, refs = refs[:n_tp], refs[n_tp:]
    gain, refs = refs[0], refs[1:]
    weights, gates, refs = refs[:4], refs[4:6], refs[6:]
    x_out, own, sends = refs[0], refs[1], refs[2 : 2 + n_dp - 1]
    acc, tail, streamed, sems = refs[-4:]
    pending = {}
    for i in range(2):
        for cols in cut(streamed.shape[2], LANES):
            copy = pltpu.make_async_copy(
                weights[2 + i].at[0, :, cols], streamed.at[i, :, cols], sems.at[len(pending)]
            )
            copy.start()
            pending[2 + i, cols.start] = copy
    me_tp, me_dp = idx[0], idx[1]
    rows = xs[0].shape[0]
    for s in range(n_tp):
        at = pl.multiple_of(peer_from(me_tp, s, n_tp) * rows, rows)
        x_out[pl.ds(at, rows), :] = xs[s][...].astype(F32)

    def arrived(i, c):
        if (i, c) in pending:
            pending[i, c].wait()

    weights = [*weights[:2], streamed.at[0], streamed.at[1]]
    project(
        x_out[...], gain[0:1, :], weights, gates, own, sends, acc, tail, me_dp, n_dp, arrived
    )


def later_kernel(n_tp, n_dp, layer, last, idx, x_prev, *refs):
    parts, refs = refs[:n_tp], refs[n_tp:]
    gain, refs = refs[0], refs[1:]
    weights, gates, refs = refs[:4], refs[4:6], refs[6:]
    x_out, own, sends, acc, tail = refs[0], refs[1], refs[2 : 1 + n_dp], *refs[1 + n_dp : 3 + n_dp]
    total = tree_sum(p[...].astype(F32) for p in parts)
    x = (x_prev[...] + total).astype(BF16).astype(F32)
    if last:
        count, x_rows = x_out.shape[0], refs[-1]
        x_rows[...] = x
        x_out[...] = x_rows[pl.ds(pl.multiple_of(idx[0] * count, count), count), :]
    else:
        x_out[...] = x
    project(x, gain[layer : layer + 1, :], weights, gates, own, sends, acc, tail, idx[1], n_dp)


def projection(idx, x_prev, pieces, layer, last, gain, weights, gates, batch, n_tp, n_dp):
    features, width = weights[0].shape[-2:]
    heads = gates[0].shape[-2]
    total = 4 * width + 2 * half_width(heads)
    rows = batch // n_dp
    out_shape = (
        [
            jax.ShapeDtypeStruct((batch // n_tp if last else batch, features), F32),
            jax.ShapeDtypeStruct((rows, total), F32),
        ]
        + [jax.ShapeDtypeStruct((rows, total), BF16)] * (n_dp - 1)
    )
    first = x_prev is None
    lead = [idx] if first else [idx, x_prev]
    body = functools.partial(first_kernel, n_tp, n_dp) if first else functools.partial(
        later_kernel, n_tp, n_dp, layer, last
    )
    in_specs = (
        [SMEM] + [VMEM] * (len(lead) - 1 + len(pieces) + 1)
        + [VMEM if w.ndim == 2 else HBM for w in (*weights, *gates)]
    )
    scratch = [
        pltpu.VMEM((batch, total), F32),
        pltpu.VMEM((batch, 2 * half_width(heads)), F32),
    ]
    if first:
        scratch += [pltpu.VMEM((2, features, width), BF16), pltpu.SemaphoreType.DMA((8,))]
    elif last:
        scratch.append(pltpu.VMEM((batch, features), F32))
    out = call(
        body, out_shape, in_specs, [VMEM] * len(out_shape), scratch, 30_000_000
    )(*lead, *pieces, gain, *weights, *gates)
    return out[0], out[1], out[2:]


def column(row, eye):
    return jnp.sum(jnp.where(eye, row, 0.0), axis=1, keepdims=True)


def spread_index(shape, j):
    lane = lax.broadcasted_iota(jnp.int32, shape, 1)
    return jnp.where(lane >= HEAD, 2 * j + 1, 2 * j)


def take_lanes(x, index):
    return jnp.take_along_axis(x, index, axis=1)


def spread_matrix(tile):
    row = lax.broadcasted_iota(jnp.int32, (LANES, 2 * LANES), 0)
    lane = lax.broadcasted_iota(jnp.int32, (LANES, 2 * LANES), 1)
    return jnp.where(row - lane // HEAD == 2 * LANES // HEAD * tile, 1.0, 0.0).astype(BF16)


def swap_matrix(outer, inner):
    size = outer * inner
    to = lax.broadcasted_iota(jnp.int32, (size, size), 0)
    source = lax.broadcasted_iota(jnp.int32, (size, size), 1)
    same = (to // inner == source % outer) & (to % inner == source // outer)
    return jnp.where(same, 1.0, 0.0).astype(BF16)


def pieces_of(x, count):
    out = []
    for _ in range(count - 1):
        high = x.astype(BF16).astype(F32)
        out.append(high)
        x = x - high
    return [*out, x]


def lanes_to_rows(x):
    low = lax.broadcasted_iota(jnp.int32, (x.shape[0], LANES), 1) < HEAD
    out = []
    for c in range(0, x.shape[1], LANES):
        chunk = x[:, c : c + LANES]
        turned = pltpu.roll(chunk, HEAD, 1)
        out += [jnp.where(low, chunk, turned), jnp.where(low, turned, chunk)]
    return jnp.concatenate(out, axis=0)


def readout_kernel(n_dp, width, heads, model, layer, *refs):
    parts, refs = refs[:n_dp], refs[n_dp:]
    bias, old_max, old_norm, memory, refs = *refs[:4], refs[4:]
    mixed_out, keep_out, admit_out, key_out, key_rows, value_rows, max_out = refs
    rows = mixed_out.shape[0]
    half = half_width(heads)
    total = tree_sum(p[...].astype(F32) for p in parts)
    tail = total[:, 4 * width :]
    tail = tail + pltpu.roll(tail, half, 1)
    inv = lax.rsqrt(tail[:, 2 * heads : 2 * heads + 1] / model + EPS)
    stored = [
        (inv * total[:, i * width : (i + 1) * width]).astype(BF16).astype(F32) for i in range(4)
    ]
    query, key = stored[0], stored[1]
    by_head = jnp.concatenate([lanes_to_rows(x) for x in stored], axis=1).astype(BF16)
    by_row = jnp.dot(swap_matrix(rows, heads), by_head, preferred_element_type=F32)
    query_rows = by_row[:, 0:LANES].astype(BF16)
    key_rows[...] = by_row[:, LANES : 2 * LANES].astype(BF16)
    value_row = by_row[:, 2 * LANES : 3 * LANES]
    value_rows[...] = value_row
    past = jnp.zeros((rows * heads, LANES), F32)
    for tile in range(HEAD * HEAD // (2 * LANES)):
        spread = jnp.dot(query_rows, spread_matrix(tile), preferred_element_type=F32)
        for c in range(0, 2 * LANES, LANES):
            at = tile * 2 * LANES + c
            block = memory[:, :, at : at + LANES].reshape(rows * heads, LANES)
            past = past + spread[:, c : c + LANES] * block
    past = past + pltpu.roll(past, HEAD, 1)

    input_pre = inv * tail[:, 0:heads]
    forget_pre = inv * tail[:, heads : 2 * heads] + bias[layer : layer + 1, :]
    log_forget = jnp.minimum(forget_pre, 0.0) - jnp.log1p(jnp.exp(-jnp.abs(forget_pre)))
    aged = log_forget + old_max[...]
    new_max = jnp.maximum(aged, input_pre)
    keep = jnp.exp(aged - new_max)
    admit = jnp.exp(input_pre - new_max) * HEAD**-0.5
    group = lax.broadcasted_iota(jnp.int32, (width, LANES), 0)
    lane = lax.broadcasted_iota(jnp.int32, (width, LANES), 1)
    head_of = jnp.where(group // HEAD == lane, 1.0, 0.0).astype(BF16)
    products = pieces_of(query * key, 2) + pieces_of(query * old_norm[...], 3)
    products.append(jnp.zeros_like(query))
    sums = jnp.dot(
        jnp.concatenate(products, axis=0).astype(BF16), head_of, preferred_element_type=F32
    )[:, 0:heads]
    query_key = sums[0:rows] + sums[rows : 2 * rows]
    query_norm = sums[2 * rows : 3 * rows] + (sums[3 * rows : 4 * rows] + sums[4 * rows : 5 * rows])
    gained = admit * query_key
    denominator = jnp.maximum(jnp.abs(keep * query_norm + gained), jnp.exp(-new_max))
    max_out[...] = new_max
    keep_out[...] = jnp.zeros_like(keep_out)
    admit_out[...] = jnp.zeros_like(admit_out)
    keep_out[:, 0:heads] = keep
    admit_out[:, 0:heads] = admit
    key_out[...] = key

    eye = lax.broadcasted_iota(jnp.int32, (heads, heads), 0) == lax.broadcasted_iota(
        jnp.int32, (heads, heads), 1
    )
    read = []
    for s in range(rows):
        at = slice(s * heads, (s + 1) * heads)
        numerator = (
            column(keep[s : s + 1], eye) * past[at] + column(gained[s : s + 1], eye) * value_row[at]
        )
        read.append(numerator / column(denominator[s : s + 1], eye))
    gate = by_row[:, 3 * LANES :]
    gated = (jnp.concatenate(read, axis=0) * jax.nn.sigmoid(gate)).astype(BF16)
    back = jnp.dot(swap_matrix(heads, rows), gated, preferred_element_type=F32)
    low = lax.broadcasted_iota(jnp.int32, (rows, LANES), 1) < HEAD
    for h in range(0, heads, 2):
        even, odd = back[h * rows : (h + 1) * rows], back[(h + 1) * rows : (h + 2) * rows]
        mixed_out[:, h * HEAD : (h + 2) * HEAD] = jnp.where(low, even, odd).astype(BF16)


def readout(parts, bias, old_max, old_norm, memory, layer, model):
    rows, heads = old_max.shape
    width = heads * HEAD
    out_shape = [
        jax.ShapeDtypeStruct((rows, width), BF16),
        jax.ShapeDtypeStruct((rows, LANES), F32),
        jax.ShapeDtypeStruct((rows, LANES), F32),
        jax.ShapeDtypeStruct((rows, width), F32),
        jax.ShapeDtypeStruct((rows * heads, LANES), BF16),
        jax.ShapeDtypeStruct((rows * heads, LANES), F32),
        jax.ShapeDtypeStruct((rows, heads), F32),
    ]
    in_specs = [VMEM] * (len(parts) + 4)
    return call(
        functools.partial(readout_kernel, len(parts), width, heads, model, layer),
        out_shape, in_specs, [VMEM] * len(out_shape), [], 20_000_000,
    )(*parts, bias, old_max, old_norm, memory)


def update_kernel(layer, *refs):
    keep_in, admit_in, key_in, key_rows, value_rows, max_in, memory, old_norm = refs[:8]
    refs = refs[8 + (3 if layer else 0) :]
    memory_out, norm_out, max_out, stage, norm, keep_rows, gain_rows, sems = refs
    rows, heads, size = memory.shape
    eye = lax.broadcasted_iota(jnp.int32, (heads, heads), 0) == lax.broadcasted_iota(
        jnp.int32, (heads, heads), 1
    )
    copies = [pltpu.make_async_copy(max_in, max_out.at[layer], sems.at[0])]
    copies[0].start()
    for j in range(heads * HEAD // LANES):
        cols = slice(j * LANES, (j + 1) * LANES)
        index = spread_index((rows, LANES), j)
        norm[:, cols] = (
            take_lanes(keep_in[...], index) * old_norm[:, cols]
            + take_lanes(admit_in[...], index) * key_in[:, cols]
        )
    copies.append(pltpu.make_async_copy(norm, norm_out.at[layer], sems.at[1]))
    copies[1].start()
    for s in range(rows):
        at = slice(s * heads, (s + 1) * heads)
        keep_rows[at] = jnp.broadcast_to(column(keep_in[s : s + 1, 0:heads], eye), (heads, LANES))
        gain_rows[at] = column(admit_in[s : s + 1, 0:heads], eye) * value_rows[at]
    tiles = size // (2 * LANES)
    group = tiles // (sems.shape[0] - 2)
    for tile in range(tiles):
        spread = jnp.dot(key_rows[...], spread_matrix(tile), preferred_element_type=F32)
        for c in range(0, 2 * LANES, LANES):
            cols = slice(tile * 2 * LANES + c, tile * 2 * LANES + c + LANES)
            block = memory[:, :, cols].reshape(rows * heads, LANES)
            fresh = keep_rows[...] * block + spread[:, c : c + LANES] * gain_rows[...]
            stage[:, :, cols] = fresh.reshape(rows, heads, LANES)
        if tile % group == group - 1:
            cols = pl.ds((tile - group + 1) * 2 * LANES, group * 2 * LANES)
            copies.append(
                pltpu.make_async_copy(
                    stage.at[:, :, cols], memory_out.at[layer, :, :, cols], sems.at[len(copies)]
                )
            )
            copies[-1].start()
    for copy in copies:
        copy.wait()


def update(read, memory, old_norm, layer, layers, earlier):
    rows, heads, size = memory.shape
    out_shape = [
        jax.ShapeDtypeStruct((layers, rows, heads, size), F32),
        jax.ShapeDtypeStruct((layers, rows, heads * HEAD), F32),
        jax.ShapeDtypeStruct((layers, rows, heads), F32),
    ]
    _, keep, admit, key, key_rows, value_rows, new_max = read
    in_specs = [VMEM] * 8 + ([HBM] * 3 if layer else [])
    return call(
        functools.partial(update_kernel, layer),
        out_shape, in_specs, [HBM] * 3,
        [
            pltpu.VMEM((rows, heads, size), F32),
            pltpu.VMEM((rows, heads * HEAD), F32),
            pltpu.VMEM((rows * heads, LANES), F32),
            pltpu.VMEM((rows * heads, LANES), F32),
            pltpu.SemaphoreType.DMA((2 + 4,)),
        ],
        20_000_000, {8: 0, 9: 1, 10: 2} if layer else None,
    )(keep, admit, key, key_rows, value_rows, new_max, memory, old_norm, *(earlier or ()))


def gather_rows(refs, me, n, scratch):
    rows = refs[0].shape[0]
    for s in range(n):
        at = pl.multiple_of(peer_from(me, s, n) * rows, rows)
        scratch[pl.ds(at, rows), :] = refs[s][...].astype(F32)
    return scratch[...].astype(BF16)


def out_kernel(n_dp, idx, *refs):
    parts, weight, out, rows = refs[:n_dp], refs[n_dp], refs[n_dp + 1], refs[n_dp + 2]
    mixed = gather_rows(parts, idx[1], n_dp, rows)
    step = min(weight.shape[1], 256)
    for c in range(0, weight.shape[1], step):
        out[:, c : c + step] = jnp.dot(
            mixed, weight[:, c : c + step], preferred_element_type=F32
        ).astype(BF16)


def last_out_kernel(n_dp, n_tp, idx, *refs):
    parts, weight, refs = refs[:n_dp], refs[n_dp], refs[n_dp + 1 :]
    own, sends, rows, acc = refs[0], refs[1 : n_tp], refs[-2], refs[-1]
    mixed = gather_rows(parts, idx[1], n_dp, rows)
    step = min(weight.shape[1], 256)
    for c in range(0, weight.shape[1], step):
        acc[:, c : c + step] = jnp.dot(mixed, weight[:, c : c + step], preferred_element_type=F32)
    count = own.shape[0]
    own[...] = acc[pl.ds(pl.multiple_of(idx[0] * count, count), count), :]
    for s in range(1, n_tp):
        at = pl.multiple_of(peer_to(idx[0], s, n_tp) * count, count)
        sends[s - 1][...] = acc[pl.ds(at, count), :].astype(BF16)


def out_projection(idx, parts, weight, n_tp, last):
    n_dp = len(parts)
    rows, width = parts[0].shape
    batch, columns = rows * n_dp, weight.shape[-1]
    in_specs = [SMEM] + [VMEM] * (n_dp + 1)
    scratch = [pltpu.VMEM((batch, width), F32)]
    if last:
        count = batch // n_tp
        out_shape = [jax.ShapeDtypeStruct((count, columns), F32)]
        out_shape += [jax.ShapeDtypeStruct((count, columns), BF16)] * (n_tp - 1)
        body = functools.partial(last_out_kernel, n_dp, n_tp)
        scratch.append(pltpu.VMEM((batch, columns), F32))
    else:
        out_shape = [jax.ShapeDtypeStruct((batch, columns), BF16)]
        body = functools.partial(out_kernel, n_dp)
    return call(
        body, out_shape, in_specs, [VMEM] * len(out_shape), scratch, 15_000_000
    )(idx, *parts, weight)


def final_add(x, parts):
    return (x + tree_sum(p.astype(F32) for p in parts)).astype(BF16)


def plain_cell(parts, bias, old_max, old_norm, memory, layer, model):
    rows, heads = old_max.shape
    width, half = heads * HEAD, half_width(heads)
    total = tree_sum(p.astype(F32) for p in parts)
    tail = total[:, 4 * width : 4 * width + half] + total[:, 4 * width + half :]
    inv = lax.rsqrt(tail[:, 2 * heads : 2 * heads + 1] / model + EPS)
    stored = lax.optimization_barrier((inv * total[:, : 4 * width]).astype(BF16)).astype(F32)
    query, key, value, gate = (
        stored[:, i * width : (i + 1) * width].reshape(rows, heads, HEAD) for i in range(4)
    )
    key = key * HEAD**-0.5
    input_pre = inv * tail[:, 0:heads]
    forget_pre = inv * tail[:, heads : 2 * heads] + bias[layer][None, :]
    aged = jax.nn.log_sigmoid(forget_pre) + old_max
    new_max = jnp.maximum(aged, input_pre)
    keep, admit = jnp.exp(aged - new_max), jnp.exp(input_pre - new_max)
    state = memory.reshape(rows, heads, HEAD, HEAD)
    state = (
        keep[:, :, None, None] * state
        + admit[:, :, None, None] * key[:, :, :, None] * value[:, :, None, :]
    )
    norm = keep[:, :, None] * old_norm.reshape(rows, heads, HEAD) + admit[:, :, None] * key
    top = jnp.einsum("bhd,bhde->bhe", query, state, precision=lax.Precision.HIGHEST)
    bottom = jnp.maximum(jnp.abs(jnp.sum(query * norm, axis=2)), jnp.exp(-new_max))
    mixed = (top / bottom[:, :, None] * jax.nn.sigmoid(gate)).astype(BF16).reshape(rows, width)
    return mixed, state.reshape(rows, heads, -1), norm.reshape(rows, width), new_max


def fills_tiles(memory):
    return memory.shape[1] % 8 == 0 and memory.shape[2] % 8 == 0


def per_device(
    n_tp, n_dp, tokens, norm_gain, query_weight, key_weight, value_weight, outgate_weight,
    input_gate_weight, forget_gate_weight, forget_bias, out_weight, memory_state,
    normalizer_state, maximum_state,
):
    layers = memory_state.shape[0]
    batch = tokens.shape[0] * n_tp
    model = query_weight.shape[1] * n_dp
    idx = jnp.stack([lax.axis_index("tp"), lax.axis_index("dp")]).astype(jnp.int32)
    weights = (query_weight, key_weight, value_weight, outgate_weight)
    gates = tuple(jnp.swapaxes(g, 1, 2) for g in (input_gate_weight, forget_gate_weight))
    x_all = None
    pieces = exchange([tokens] * (n_tp - 1), "tp", n_tp)
    own, gain, *used = load((tokens, norm_gain), (*gates, *weights[:2]), 0)
    used += [in_hbm(w) for w in weights[2:]]
    pieces = [own] + pieces
    tiled = fills_tiles(memory_state)
    states, plain = None, []
    for layer in range(layers):
        last = layer == layers - 1
        x_all, own, sends = projection(
            idx, x_all, pieces, layer, last, gain, used[2:], used[:2], batch, n_tp, n_dp
        )
        parts = [own] + exchange(sends, "dp", n_dp)
        bias, old_max, old_norm, memory, project_out = load(
            (forget_bias,), (maximum_state, normalizer_state, memory_state, out_weight),
            layer,
        )
        if tiled:
            read = readout(parts, bias, old_max, old_norm, memory, layer, model)
            mixed = read[0]
        else:
            mixed, *rest = plain_cell(parts, bias, old_max, old_norm, memory, layer, model)
            plain.append(rest)
        mixes = [mixed] + exchange([mixed] * (n_dp - 1), "dp", n_dp)
        if tiled:
            states = update(read, memory, old_norm, layer, layers, states)
        part = out_projection(idx, mixes, project_out, n_tp, last)
        sends = part[1:] if last else [part[0]] * (n_tp - 1)
        pieces = [part[0]] + exchange(sends, "tp", n_tp)
        if not last:
            used = load((), (*gates, *weights), layer + 1)
    next_tokens = final_add(x_all, pieces)
    if plain:
        states = [jnp.stack(column) for column in zip(*plain)]
    return (next_tokens, *states)


def solution(mesh):
    sizes = dict(mesh.shape)
    in_specs = (
        P(("grp", "tp"), "dp"),
        P(None, "dp"),
        P(None, "dp", "tp"),
        P(None, "dp", "tp"),
        P(None, "dp", "tp"),
        P(None, "dp", "tp"),
        P(None, "dp", "tp"),
        P(None, "dp", "tp"),
        P(None, "tp"),
        P(None, "tp", "dp"),
        P(None, ("grp", "dp"), "tp", None),
        P(None, ("grp", "dp"), "tp"),
        P(None, ("grp", "dp"), "tp"),
    )
    out_specs = (
        P(("grp", "tp"), "dp"),
        P(None, ("grp", "dp"), "tp", None),
        P(None, ("grp", "dp"), "tp"),
        P(None, ("grp", "dp"), "tp"),
    )
    n_tp, n_dp = sizes["tp"], sizes["dp"]

    def whole(*args):
        return per_device(n_tp, n_dp, *args)

    def step(*args):
        sharded = jax.shard_map(
            whole, mesh=mesh, in_specs=in_specs, out_specs=out_specs, check_vma=False
        )
        return sharded(*args)

    return step
```

```python
import functools
import math

import jax
import jax.numpy as jnp
from jax import lax
from jax.experimental import pallas as pl
from jax.experimental.pallas import tpu as pltpu
from jax.sharding import PartitionSpec as P


HEAD = 64
LANES = 128
EPS = 1e-06
F32 = jnp.float32
BF16 = jnp.bfloat16
VMEM_LIMIT = 10 * 1024 * 1024
LOAD_FLOPS = 30_000_000


def is_pow2(n):
    return n & (n - 1) == 0


def peer_to(me, step, n):
    return me ^ step if is_pow2(n) else lax.rem(me + step, n)


def peer_from(me, step, n):
    return me ^ step if is_pow2(n) else lax.rem(me + n - step, n)


def exchange(blocks, axis, n):
    out = {}
    for s in reversed(range(1, n)):
        pairs = [(i, i ^ s if is_pow2(n) else (i + s) % n) for i in range(n)]
        out[s] = lax.ppermute(blocks[s - 1], axis, pairs)
    return [out[s] for s in range(1, n)]


def tree_sum(terms):
    terms = list(terms)
    while len(terms) > 1:
        nxt = [a + b for a, b in zip(terms[0::2], terms[1::2])]
        if len(terms) % 2:
            nxt.append(terms[-1])
        terms = nxt
    return terms[0]


def call(body, out_shape, in_specs, out_specs, scratch, flops, aliases=None):
    return pl.pallas_call(
        body,
        grid=(1,),
        out_shape=out_shape,
        in_specs=in_specs,
        out_specs=out_specs,
        scratch_shapes=scratch,
        input_output_aliases=aliases or {},
        compiler_params=pltpu.CompilerParams(vmem_limit_bytes=VMEM_LIMIT),
        cost_estimate=pl.CostEstimate(flops=flops, bytes_accessed=1 << 20, transcendentals=0),
    )


VMEM = pl.BlockSpec(memory_space=pltpu.VMEM)
ANY = pl.BlockSpec(memory_space=pl.ANY)
HBM = pl.BlockSpec(memory_space=pltpu.HBM)


def half_width(heads):
    return -(-(2 * heads + 1) // 64) * 64


def project(x, gain, weights, gates, own_ref, send_refs, acc, tail, me_dp, n_dp):
    batch = x.shape[0]
    width = weights[0].shape[1]
    heads = gates[0].shape[0]
    half = half_width(heads)
    scaled = (x * gain).astype(BF16)
    tail[...] = jnp.zeros_like(tail)
    for i in range(2):
        tail[:, i * heads : (i + 1) * heads] = lax.dot_general(
            scaled, gates[i][...], (((1,), (1,)), ((), ())), preferred_element_type=F32
        )
    tail[:, 2 * heads : 2 * heads + 1] = jnp.sum(x * x, axis=1, keepdims=True)
    full = tail[...]
    high = full.astype(BF16).astype(F32)
    acc[:, 4 * width :] = high + pltpu.roll(full - high, half, 1)
    step = min(width, 256)
    for i in range(4):
        for c in range(0, width, step):
            acc[:, i * width + c : i * width + c + step] = jnp.dot(
                scaled, weights[i][:, c : c + step], preferred_element_type=F32
            )
    rows = batch // n_dp
    own_ref[...] = acc[pl.ds(pl.multiple_of(me_dp * rows, rows), rows), :]
    for s in range(1, n_dp):
        to = peer_to(me_dp, s, n_dp)
        send_refs[s - 1][...] = acc[pl.ds(pl.multiple_of(to * rows, rows), rows), :].astype(BF16)


def cut(extent, unit):
    count = next((n for n in (4, 2) if extent % (n * unit) == 0), 1)
    return [slice(i * extent // count, (i + 1) * extent // count) for i in range(count)]


def load_plan(shape, dtype):
    large = math.prod(shape) * jnp.dtype(dtype).itemsize >= 1 << 19
    return cut(shape[0], 1 if len(shape) > 2 else 16) if large else [slice(0, shape[0])]


def load_kernel(layers, *refs):
    count = len(layers)
    sources, outs, sems = refs[:count], refs[count:-1], refs[-1]
    copies = []
    for source, out, layer in zip(sources, outs, layers):
        whole = source if layer is None else source.at[layer]
        for rows in load_plan(out.shape, out.dtype):
            sem = sems.at[len(copies)]
            copies.append(pltpu.make_async_copy(whole.at[rows], out.at[rows], sem))
            copies[-1].start()
    for copy in copies:
        copy.wait()


def in_hbm(array):
    return pltpu.with_memory_space_constraint(array, pltpu.HBM)


def load(flat, stacked, layer):
    layers = [None] * len(flat) + [layer] * len(stacked)
    shapes = [(w.shape, w.dtype) for w in flat] + [(w.shape[1:], w.dtype) for w in stacked]
    count = sum(len(load_plan(*entry)) for entry in shapes)
    return call(
        functools.partial(load_kernel, layers),
        [jax.ShapeDtypeStruct(shape, dtype) for shape, dtype in shapes],
        [HBM] * len(layers), [VMEM] * len(shapes),
        [pltpu.SemaphoreType.DMA((count,))], LOAD_FLOPS,
    )(*[in_hbm(w) for w in (*flat, *stacked)])


def first_kernel(n_tp, n_dp, *refs):
    xs, refs = refs[:n_tp], refs[n_tp:]
    gain, refs = refs[0], refs[1:]
    weights, gates, refs = refs[:4], refs[4:6], refs[6:]
    x_out, own, sends = refs[0], refs[1], refs[2 : 2 + n_dp - 1]
    acc, tail = refs[-2:]
    me_tp, me_dp = lax.axis_index("tp"), lax.axis_index("dp")
    rows = xs[0].shape[0]
    for s in range(n_tp):
        at = pl.multiple_of(peer_from(me_tp, s, n_tp) * rows, rows)
        x_out[pl.ds(at, rows), :] = xs[s][...].astype(F32)
    project(x_out[...], gain[0:1, :], weights, gates, own, sends, acc, tail, me_dp, n_dp)


def later_kernel(n_tp, n_dp, layer, last, x_prev, *refs):
    me_tp, me_dp = lax.axis_index("tp"), lax.axis_index("dp")
    parts, refs = refs[:n_tp], refs[n_tp:]
    gain, refs = refs[0], refs[1:]
    weights, gates, refs = refs[:4], refs[4:6], refs[6:]
    x_out, own, sends, acc, tail = refs[0], refs[1], refs[2 : 1 + n_dp], *refs[1 + n_dp : 3 + n_dp]
    total = tree_sum(p[...].astype(F32) for p in parts)
    x = (x_prev[...] + total).astype(BF16).astype(F32)
    if last:
        count, x_rows = x_out.shape[0], refs[-1]
        x_rows[...] = x
        x_out[...] = x_rows[pl.ds(pl.multiple_of(me_tp * count, count), count), :]
    else:
        x_out[...] = x
    project(x, gain[layer : layer + 1, :], weights, gates, own, sends, acc, tail, me_dp, n_dp)


def projection(x_prev, pieces, layer, last, gain, weights, gates, batch, n_tp, n_dp):
    features, width = weights[0].shape[-2:]
    heads = gates[0].shape[-2]
    total = 4 * width + 2 * half_width(heads)
    rows = batch // n_dp
    out_shape = (
        [
            jax.ShapeDtypeStruct((batch // n_tp if last else batch, features), F32),
            jax.ShapeDtypeStruct((rows, total), F32),
        ]
        + [jax.ShapeDtypeStruct((rows, total), BF16)] * (n_dp - 1)
    )
    first = x_prev is None
    lead = [] if first else [x_prev]
    body = functools.partial(first_kernel, n_tp, n_dp) if first else functools.partial(
        later_kernel, n_tp, n_dp, layer, last
    )
    in_specs = (
        [VMEM] * (len(lead) + len(pieces) + 1)
        + [VMEM] * (len(weights) + len(gates))
    )
    scratch = [
        pltpu.VMEM((batch, total), F32),
        pltpu.VMEM((batch, 2 * half_width(heads)), F32),
    ]
    if last:
        scratch.append(pltpu.VMEM((batch, features), F32))
    out = call(
        body, out_shape, in_specs, [VMEM] * len(out_shape), scratch, 30_000_000
    )(*lead, *pieces, gain, *weights, *gates)
    return out[0], out[1], out[2:]


def column(row, eye):
    return jnp.sum(jnp.where(eye, row, 0.0), axis=1, keepdims=True)


def spread_index(shape, j):
    lane = lax.broadcasted_iota(jnp.int32, shape, 1)
    return jnp.where(lane >= HEAD, 2 * j + 1, 2 * j)


def take_lanes(x, index):
    return jnp.take_along_axis(x, index, axis=1)


def spread_matrix(tile):
    row = lax.broadcasted_iota(jnp.int32, (LANES, 2 * LANES), 0)
    lane = lax.broadcasted_iota(jnp.int32, (LANES, 2 * LANES), 1)
    return jnp.where(row - lane // HEAD == 2 * LANES // HEAD * tile, 1.0, 0.0).astype(BF16)


def swap_matrix(outer, inner):
    size = outer * inner
    to = lax.broadcasted_iota(jnp.int32, (size, size), 0)
    source = lax.broadcasted_iota(jnp.int32, (size, size), 1)
    same = (to // inner == source % outer) & (to % inner == source // outer)
    return jnp.where(same, 1.0, 0.0).astype(BF16)


def pieces_of(x, count):
    out = []
    for _ in range(count - 1):
        high = x.astype(BF16).astype(F32)
        out.append(high)
        x = x - high
    return [*out, x]


def lanes_to_rows(x):
    low = lax.broadcasted_iota(jnp.int32, (x.shape[0], LANES), 1) < HEAD
    out = []
    for c in range(0, x.shape[1], LANES):
        chunk = x[:, c : c + LANES]
        turned = pltpu.roll(chunk, HEAD, 1)
        out += [jnp.where(low, chunk, turned), jnp.where(low, turned, chunk)]
    return jnp.concatenate(out, axis=0)


def readout_kernel(n_dp, width, heads, model, layer, *refs):
    parts, refs = refs[:n_dp], refs[n_dp:]
    bias, old_max, old_norm, memory, refs = *refs[:4], refs[4:]
    mixed_out, keep_out, admit_out, key_out, key_rows, value_rows, max_out = refs
    rows = mixed_out.shape[0]
    half = half_width(heads)
    total = tree_sum(p[...].astype(F32) for p in parts)
    tail = total[:, 4 * width :]
    tail = tail + pltpu.roll(tail, half, 1)
    inv = lax.rsqrt(tail[:, 2 * heads : 2 * heads + 1] / model + EPS)
    stored = [
        (inv * total[:, i * width : (i + 1) * width]).astype(BF16).astype(F32) for i in range(4)
    ]
    query, key = stored[0], stored[1]
    by_head = jnp.concatenate([lanes_to_rows(x) for x in stored], axis=1).astype(BF16)
    by_row = jnp.dot(swap_matrix(rows, heads), by_head, preferred_element_type=F32)
    query_rows = by_row[:, 0:LANES].astype(BF16)
    key_rows[...] = by_row[:, LANES : 2 * LANES].astype(BF16)
    value_row = by_row[:, 2 * LANES : 3 * LANES]
    value_rows[...] = value_row
    past = jnp.zeros((rows * heads, LANES), F32)
    for tile in range(HEAD * HEAD // (2 * LANES)):
        spread = jnp.dot(query_rows, spread_matrix(tile), preferred_element_type=F32)
        for c in range(0, 2 * LANES, LANES):
            at = tile * 2 * LANES + c
            block = memory[:, :, at : at + LANES].reshape(rows * heads, LANES)
            past = past + spread[:, c : c + LANES] * block
    past = past + pltpu.roll(past, HEAD, 1)

    input_pre = inv * tail[:, 0:heads]
    forget_pre = inv * tail[:, heads : 2 * heads] + bias[layer : layer + 1, :]
    log_forget = jnp.minimum(forget_pre, 0.0) - jnp.log1p(jnp.exp(-jnp.abs(forget_pre)))
    aged = log_forget + old_max[...]
    new_max = jnp.maximum(aged, input_pre)
    keep = jnp.exp(aged - new_max)
    admit = jnp.exp(input_pre - new_max) * HEAD**-0.5
    group = lax.broadcasted_iota(jnp.int32, (width, LANES), 0)
    lane = lax.broadcasted_iota(jnp.int32, (width, LANES), 1)
    head_of = jnp.where(group // HEAD == lane, 1.0, 0.0).astype(BF16)
    products = pieces_of(query * key, 2) + pieces_of(query * old_norm[...], 3)
    products.append(jnp.zeros_like(query))
    sums = jnp.dot(
        jnp.concatenate(products, axis=0).astype(BF16), head_of, preferred_element_type=F32
    )[:, 0:heads]
    query_key = sums[0:rows] + sums[rows : 2 * rows]
    query_norm = sums[2 * rows : 3 * rows] + (sums[3 * rows : 4 * rows] + sums[4 * rows : 5 * rows])
    gained = admit * query_key
    denominator = jnp.maximum(jnp.abs(keep * query_norm + gained), jnp.exp(-new_max))
    max_out[...] = new_max
    keep_out[...] = jnp.zeros_like(keep_out)
    admit_out[...] = jnp.zeros_like(admit_out)
    keep_out[:, 0:heads] = keep
    admit_out[:, 0:heads] = admit
    key_out[...] = key

    eye = lax.broadcasted_iota(jnp.int32, (heads, heads), 0) == lax.broadcasted_iota(
        jnp.int32, (heads, heads), 1
    )
    read = []
    for s in range(rows):
        at = slice(s * heads, (s + 1) * heads)
        numerator = (
            column(keep[s : s + 1], eye) * past[at] + column(gained[s : s + 1], eye) * value_row[at]
        )
        read.append(numerator / column(denominator[s : s + 1], eye))
    gate = by_row[:, 3 * LANES :]
    gated = (jnp.concatenate(read, axis=0) * jax.nn.sigmoid(gate)).astype(BF16)
    back = jnp.dot(swap_matrix(heads, rows), gated, preferred_element_type=F32)
    low = lax.broadcasted_iota(jnp.int32, (rows, LANES), 1) < HEAD
    for h in range(0, heads, 2):
        even, odd = back[h * rows : (h + 1) * rows], back[(h + 1) * rows : (h + 2) * rows]
        mixed_out[:, h * HEAD : (h + 2) * HEAD] = jnp.where(low, even, odd).astype(BF16)


def readout(parts, bias, old_max, old_norm, memory, layer, model):
    rows, heads = old_max.shape
    width = heads * HEAD
    out_shape = [
        jax.ShapeDtypeStruct((rows, width), BF16),
        jax.ShapeDtypeStruct((rows, LANES), F32),
        jax.ShapeDtypeStruct((rows, LANES), F32),
        jax.ShapeDtypeStruct((rows, width), F32),
        jax.ShapeDtypeStruct((rows * heads, LANES), BF16),
        jax.ShapeDtypeStruct((rows * heads, LANES), F32),
        jax.ShapeDtypeStruct((rows, heads), F32),
    ]
    in_specs = [VMEM] * (len(parts) + 4)
    return call(
        functools.partial(readout_kernel, len(parts), width, heads, model, layer),
        out_shape, in_specs, [VMEM] * len(out_shape), [], 20_000_000,
    )(*parts, bias, old_max, old_norm, memory)


def update_kernel(layer, *refs):
    keep_in, admit_in, key_in, key_rows, value_rows, max_in, memory, old_norm = refs[:8]
    refs = refs[8 + (3 if layer else 0) :]
    memory_out, norm_out, max_out, stage, norm, keep_rows, gain_rows, sems = refs
    rows, heads, size = memory.shape
    eye = lax.broadcasted_iota(jnp.int32, (heads, heads), 0) == lax.broadcasted_iota(
        jnp.int32, (heads, heads), 1
    )
    copies = [pltpu.make_async_copy(max_in, max_out.at[layer], sems.at[0])]
    copies[0].start()
    for j in range(heads * HEAD // LANES):
        cols = slice(j * LANES, (j + 1) * LANES)
        index = spread_index((rows, LANES), j)
        norm[:, cols] = (
            take_lanes(keep_in[...], index) * old_norm[:, cols]
            + take_lanes(admit_in[...], index) * key_in[:, cols]
        )
    copies.append(pltpu.make_async_copy(norm, norm_out.at[layer], sems.at[1]))
    copies[1].start()
    for s in range(rows):
        at = slice(s * heads, (s + 1) * heads)
        keep_rows[at] = jnp.broadcast_to(column(keep_in[s : s + 1, 0:heads], eye), (heads, LANES))
        gain_rows[at] = column(admit_in[s : s + 1, 0:heads], eye) * value_rows[at]
    tiles = size // (2 * LANES)
    group = tiles // (sems.shape[0] - 2)
    for tile in range(tiles):
        spread = jnp.dot(key_rows[...], spread_matrix(tile), preferred_element_type=F32)
        for c in range(0, 2 * LANES, LANES):
            cols = slice(tile * 2 * LANES + c, tile * 2 * LANES + c + LANES)
            block = memory[:, :, cols].reshape(rows * heads, LANES)
            fresh = keep_rows[...] * block + spread[:, c : c + LANES] * gain_rows[...]
            stage[:, :, cols] = fresh.reshape(rows, heads, LANES)
        if tile % group == group - 1:
            cols = pl.ds((tile - group + 1) * 2 * LANES, group * 2 * LANES)
            copies.append(
                pltpu.make_async_copy(
                    stage.at[:, :, cols], memory_out.at[layer, :, :, cols], sems.at[len(copies)]
                )
            )
            copies[-1].start()
    for copy in copies:
        copy.wait()


def update(read, memory, old_norm, layer, layers, earlier):
    rows, heads, size = memory.shape
    out_shape = [
        jax.ShapeDtypeStruct((layers, rows, heads, size), F32),
        jax.ShapeDtypeStruct((layers, rows, heads * HEAD), F32),
        jax.ShapeDtypeStruct((layers, rows, heads), F32),
    ]
    _, keep, admit, key, key_rows, value_rows, new_max = read
    in_specs = [VMEM] * 8 + ([HBM] * 3 if layer else [])
    return call(
        functools.partial(update_kernel, layer),
        out_shape, in_specs, [HBM] * 3,
        [
            pltpu.VMEM((rows, heads, size), F32),
            pltpu.VMEM((rows, heads * HEAD), F32),
            pltpu.VMEM((rows * heads, LANES), F32),
            pltpu.VMEM((rows * heads, LANES), F32),
            pltpu.SemaphoreType.DMA((2 + 4,)),
        ],
        20_000_000, {8: 0, 9: 1, 10: 2} if layer else None,
    )(keep, admit, key, key_rows, value_rows, new_max, memory, old_norm, *(earlier or ()))


def gather_rows(refs, me, n, scratch):
    rows = refs[0].shape[0]
    for s in range(n):
        at = pl.multiple_of(peer_from(me, s, n) * rows, rows)
        scratch[pl.ds(at, rows), :] = refs[s][...].astype(F32)
    return scratch[...].astype(BF16)


def out_kernel(n_dp, *refs):
    parts, weight, out, rows = refs[:n_dp], refs[n_dp], refs[n_dp + 1], refs[n_dp + 2]
    mixed = gather_rows(parts, lax.axis_index("dp"), n_dp, rows)
    step = min(weight.shape[1], 256)
    for c in range(0, weight.shape[1], step):
        out[:, c : c + step] = jnp.dot(
            mixed, weight[:, c : c + step], preferred_element_type=F32
        ).astype(BF16)


def last_out_kernel(n_dp, n_tp, *refs):
    me_tp = lax.axis_index("tp")
    parts, weight, refs = refs[:n_dp], refs[n_dp], refs[n_dp + 1 :]
    own, sends, rows, acc = refs[0], refs[1 : n_tp], refs[-2], refs[-1]
    mixed = gather_rows(parts, lax.axis_index("dp"), n_dp, rows)
    step = min(weight.shape[1], 256)
    for c in range(0, weight.shape[1], step):
        acc[:, c : c + step] = jnp.dot(mixed, weight[:, c : c + step], preferred_element_type=F32)
    count = own.shape[0]
    own[...] = acc[pl.ds(pl.multiple_of(me_tp * count, count), count), :]
    for s in range(1, n_tp):
        at = pl.multiple_of(peer_to(me_tp, s, n_tp) * count, count)
        sends[s - 1][...] = acc[pl.ds(at, count), :].astype(BF16)


def out_projection(parts, weight, n_tp, last):
    n_dp = len(parts)
    rows, width = parts[0].shape
    batch, columns = rows * n_dp, weight.shape[-1]
    in_specs = [VMEM] * (n_dp + 1)
    scratch = [pltpu.VMEM((batch, width), F32)]
    if last:
        count = batch // n_tp
        out_shape = [jax.ShapeDtypeStruct((count, columns), F32)]
        out_shape += [jax.ShapeDtypeStruct((count, columns), BF16)] * (n_tp - 1)
        body = functools.partial(last_out_kernel, n_dp, n_tp)
        scratch.append(pltpu.VMEM((batch, columns), F32))
    else:
        out_shape = [jax.ShapeDtypeStruct((batch, columns), BF16)]
        body = functools.partial(out_kernel, n_dp)
    return call(
        body, out_shape, in_specs, [VMEM] * len(out_shape), scratch, 15_000_000
    )(*parts, weight)


def final_add(x, parts):
    return (x + tree_sum(p.astype(F32) for p in parts)).astype(BF16)


def plain_cell(parts, bias, old_max, old_norm, memory, layer, model):
    rows, heads = old_max.shape
    width, half = heads * HEAD, half_width(heads)
    total = tree_sum(p.astype(F32) for p in parts)
    tail = total[:, 4 * width : 4 * width + half] + total[:, 4 * width + half :]
    inv = lax.rsqrt(tail[:, 2 * heads : 2 * heads + 1] / model + EPS)
    stored = lax.optimization_barrier((inv * total[:, : 4 * width]).astype(BF16)).astype(F32)
    query, key, value, gate = (
        stored[:, i * width : (i + 1) * width].reshape(rows, heads, HEAD) for i in range(4)
    )
    key = key * HEAD**-0.5
    input_pre = inv * tail[:, 0:heads]
    forget_pre = inv * tail[:, heads : 2 * heads] + bias[layer][None, :]
    aged = jax.nn.log_sigmoid(forget_pre) + old_max
    new_max = jnp.maximum(aged, input_pre)
    keep, admit = jnp.exp(aged - new_max), jnp.exp(input_pre - new_max)
    state = memory.reshape(rows, heads, HEAD, HEAD)
    state = (
        keep[:, :, None, None] * state
        + admit[:, :, None, None] * key[:, :, :, None] * value[:, :, None, :]
    )
    norm = keep[:, :, None] * old_norm.reshape(rows, heads, HEAD) + admit[:, :, None] * key
    top = jnp.einsum("bhd,bhde->bhe", query, state, precision=lax.Precision.HIGHEST)
    bottom = jnp.maximum(jnp.abs(jnp.sum(query * norm, axis=2)), jnp.exp(-new_max))
    mixed = (top / bottom[:, :, None] * jax.nn.sigmoid(gate)).astype(BF16).reshape(rows, width)
    return mixed, state.reshape(rows, heads, -1), norm.reshape(rows, width), new_max


def fills_tiles(memory):
    return memory.shape[1] % 8 == 0 and memory.shape[2] % 8 == 0


def per_device(
    n_tp, n_dp, tokens, norm_gain, query_weight, key_weight, value_weight, outgate_weight,
    input_gate_weight, forget_gate_weight, forget_bias, out_weight, memory_state,
    normalizer_state, maximum_state,
):
    layers = memory_state.shape[0]
    batch = tokens.shape[0] * n_tp
    model = query_weight.shape[1] * n_dp
    weights = (query_weight, key_weight, value_weight, outgate_weight)
    gates = tuple(jnp.swapaxes(g, 1, 2) for g in (input_gate_weight, forget_gate_weight))
    x_all = None
    pieces = exchange([tokens] * (n_tp - 1), "tp", n_tp)
    own, gain, *used = load((tokens, norm_gain), (*gates, *weights), 0)
    pieces = [own] + pieces
    tiled = fills_tiles(memory_state)
    states, plain = None, []
    for layer in range(layers):
        last = layer == layers - 1
        x_all, own, sends = projection(
            x_all, pieces, layer, last, gain, used[2:], used[:2], batch, n_tp, n_dp
        )
        parts = [own] + exchange(sends, "dp", n_dp)
        bias, old_max, old_norm, memory, project_out = load(
            (forget_bias,), (maximum_state, normalizer_state, memory_state, out_weight),
            layer,
        )
        if tiled:
            read = readout(parts, bias, old_max, old_norm, memory, layer, model)
            mixed = read[0]
        else:
            mixed, *rest = plain_cell(parts, bias, old_max, old_norm, memory, layer, model)
            plain.append(rest)
        mixes = [mixed] + exchange([mixed] * (n_dp - 1), "dp", n_dp)
        if tiled:
            states = update(read, memory, old_norm, layer, layers, states)
        part = out_projection(mixes, project_out, n_tp, last)
        sends = part[1:] if last else [part[0]] * (n_tp - 1)
        pieces = [part[0]] + exchange(sends, "tp", n_tp)
        if not last:
            used = load((), (*gates, *weights), layer + 1)
    next_tokens = final_add(x_all, pieces)
    if plain:
        states = [jnp.stack(column) for column in zip(*plain)]
    return (next_tokens, *states)


def solution(mesh):
    sizes = dict(mesh.shape)
    in_specs = (
        P(("grp", "tp"), "dp"),
        P(None, "dp"),
        P(None, "dp", "tp"),
        P(None, "dp", "tp"),
        P(None, "dp", "tp"),
        P(None, "dp", "tp"),
        P(None, "dp", "tp"),
        P(None, "dp", "tp"),
        P(None, "tp"),
        P(None, "tp", "dp"),
        P(None, ("grp", "dp"), "tp", None),
        P(None, ("grp", "dp"), "tp"),
        P(None, ("grp", "dp"), "tp"),
    )
    out_specs = (
        P(("grp", "tp"), "dp"),
        P(None, ("grp", "dp"), "tp", None),
        P(None, ("grp", "dp"), "tp"),
        P(None, ("grp", "dp"), "tp"),
    )
    n_tp, n_dp = sizes["tp"], sizes["dp"]

    def whole(*args):
        return per_device(n_tp, n_dp, *args)

    def step(*args):
        sharded = jax.shard_map(
            whole, mesh=mesh, in_specs=in_specs, out_specs=out_specs, check_vma=False
        )
        return sharded(*args)

    return step
```

```python
import functools
import math

import jax
import jax.numpy as jnp
from jax import lax
from jax.experimental import pallas as pl
from jax.experimental.pallas import tpu as pltpu
from jax.sharding import PartitionSpec as P


HEAD = 64
LANES = 128
EPS = 1e-06
F32 = jnp.float32
BF16 = jnp.bfloat16
VMEM_LIMIT = 10 * 1024 * 1024
LOAD_FLOPS = 30_000_000


def is_pow2(n):
    return n & (n - 1) == 0


def peer_to(me, step, n):
    return me ^ step if is_pow2(n) else lax.rem(me + step, n)


def peer_from(me, step, n):
    return me ^ step if is_pow2(n) else lax.rem(me + n - step, n)


def place_of(block, me, n):
    return block ^ me if is_pow2(n) else lax.rem(block + n - me, n)


def exchange(blocks, axis, n):
    out = {}
    for s in reversed(range(1, n)):
        pairs = [(i, i ^ s if is_pow2(n) else (i + s) % n) for i in range(n)]
        out[s] = lax.ppermute(blocks[s - 1], axis, pairs)
    return [out[s] for s in range(1, n)]


def tree_sum(terms):
    terms = list(terms)
    while len(terms) > 1:
        nxt = [a + b for a, b in zip(terms[0::2], terms[1::2])]
        if len(terms) % 2:
            nxt.append(terms[-1])
        terms = nxt
    return terms[0]


def call(body, out_shape, in_specs, out_specs, scratch, flops, aliases=None):
    return pl.pallas_call(
        body,
        grid=(1,),
        out_shape=out_shape,
        in_specs=in_specs,
        out_specs=out_specs,
        scratch_shapes=scratch,
        input_output_aliases=aliases or {},
        compiler_params=pltpu.CompilerParams(vmem_limit_bytes=VMEM_LIMIT),
        cost_estimate=pl.CostEstimate(flops=flops, bytes_accessed=1 << 20, transcendentals=0),
    )


VMEM = pl.BlockSpec(memory_space=pltpu.VMEM)
ANY = pl.BlockSpec(memory_space=pl.ANY)
HBM = pl.BlockSpec(memory_space=pltpu.HBM)


def half_width(heads):
    return -(-(2 * heads + 1) // 64) * 64


def project(x, gain, weights, gates, own_ref, send_refs, tail):
    width = weights[0].shape[1]
    heads = gates[0].shape[0]
    rows = own_ref.shape[0]
    scaled = (x * gain).astype(BF16)

    def put(value, at):
        cols = slice(at, at + value.shape[1])
        own_ref[:, cols] = value[0:rows]
        for s, ref in enumerate(send_refs):
            ref[:, cols] = value[(s + 1) * rows : (s + 2) * rows].astype(ref.dtype)

    tail[...] = jnp.zeros_like(tail)
    for i in range(2):
        tail[:, i * heads : (i + 1) * heads] = lax.dot_general(
            scaled, gates[i][...], (((1,), (1,)), ((), ())), preferred_element_type=F32
        )
    tail[:, 2 * heads : 2 * heads + 1] = jnp.sum(x * x, axis=1, keepdims=True)
    full = tail[...]
    high = full.astype(BF16).astype(F32)
    put(high + pltpu.roll(full - high, half_width(heads), 1), 4 * width)
    step = min(width, 256)
    for i in range(4):
        for c in range(0, width, step):
            value = jnp.dot(scaled, weights[i][:, c : c + step], preferred_element_type=F32)
            put(value, i * width + c)


def cut(extent, unit):
    count = next((n for n in (4, 2) if extent % (n * unit) == 0), 1)
    return [slice(i * extent // count, (i + 1) * extent // count) for i in range(count)]


def load_plan(shape, dtype):
    large = math.prod(shape) * jnp.dtype(dtype).itemsize >= 1 << 19
    return cut(shape[0], 1 if len(shape) > 2 else 16) if large else [slice(0, shape[0])]


def load_kernel(layers, *refs):
    count = len(layers)
    sources, outs, sems = refs[:count], refs[count:-1], refs[-1]
    copies = []
    for source, out, layer in zip(sources, outs, layers):
        whole = source if layer is None else source.at[layer]
        for rows in load_plan(out.shape, out.dtype):
            sem = sems.at[len(copies)]
            copies.append(pltpu.make_async_copy(whole.at[rows], out.at[rows], sem))
            copies[-1].start()
    for copy in copies:
        copy.wait()


def in_hbm(array):
    return pltpu.with_memory_space_constraint(array, pltpu.HBM)


def load(flat, stacked, layer):
    layers = [None] * len(flat) + [layer] * len(stacked)
    shapes = [(w.shape, w.dtype) for w in flat] + [(w.shape[1:], w.dtype) for w in stacked]
    count = sum(len(load_plan(*entry)) for entry in shapes)
    return call(
        functools.partial(load_kernel, layers),
        [jax.ShapeDtypeStruct(shape, dtype) for shape, dtype in shapes],
        [HBM] * len(layers), [VMEM] * len(shapes),
        [pltpu.SemaphoreType.DMA((count,))], LOAD_FLOPS,
    )(*[in_hbm(w) for w in (*flat, *stacked)])


def first_kernel(n_tp, n_dp, *refs):
    xs, refs = refs[:n_tp], refs[n_tp:]
    gain, weights, gates, refs = refs[0], refs[1:5], refs[5:7], refs[7:]
    x_out, own, sends, tail = refs[0], refs[1], refs[2 : 1 + n_dp], refs[-1]
    me_tp, me_dp = lax.axis_index("tp"), lax.axis_index("dp")
    rows = xs[0].shape[0]
    for s in range(n_tp):
        place = place_of(peer_from(me_tp, s, n_tp), me_dp, n_dp)
        x_out[pl.ds(pl.multiple_of(place * rows, rows), rows), :] = xs[s][...].astype(F32)
    project(x_out[...], gain[0:1, :], weights, gates, own, sends, tail)


def later_kernel(n_tp, n_dp, layer, last, x_prev, *refs):
    parts, refs = refs[:n_tp], refs[n_tp:]
    gain, weights, gates, refs = refs[0], refs[1:5], refs[5:7], refs[7:]
    x_out, own, sends, tail = refs[0], refs[1], refs[2 : 1 + n_dp], refs[1 + n_dp]
    total = tree_sum(p[...].astype(F32) for p in parts)
    x = (x_prev[...] + total).astype(BF16).astype(F32)
    if last:
        count, x_rows = x_out.shape[0], refs[-1]
        place = place_of(lax.axis_index("tp"), lax.axis_index("dp"), n_dp)
        x_rows[...] = x
        x_out[...] = x_rows[pl.ds(pl.multiple_of(place * count, count), count), :]
    else:
        x_out[...] = x
    project(x, gain[layer : layer + 1, :], weights, gates, own, sends, tail)


def projection(x_prev, pieces, layer, last, gain, weights, gates, batch, n_tp, n_dp):
    features, width = weights[0].shape[-2:]
    heads = gates[0].shape[-2]
    total = 4 * width + 2 * half_width(heads)
    rows = batch // n_dp
    out_shape = (
        [
            jax.ShapeDtypeStruct((batch // n_tp if last else batch, features), F32),
            jax.ShapeDtypeStruct((rows, total), F32),
        ]
        + [jax.ShapeDtypeStruct((rows, total), F32 if s == 1 else BF16) for s in range(1, n_dp)]
    )
    first = x_prev is None
    lead = [] if first else [x_prev]
    body = functools.partial(first_kernel, n_tp, n_dp) if first else functools.partial(
        later_kernel, n_tp, n_dp, layer, last
    )
    in_specs = (
        [VMEM] * (len(lead) + len(pieces) + 1)
        + [VMEM] * (len(weights) + len(gates))
    )
    scratch = [pltpu.VMEM((batch, 2 * half_width(heads)), F32)]
    if last:
        scratch.append(pltpu.VMEM((batch, features), F32))
    out = call(
        body, out_shape, in_specs, [VMEM] * len(out_shape), scratch, 30_000_000
    )(*lead, *pieces, gain, *weights, *gates)
    return out[0], out[1], out[2:]


def column(row, eye):
    return jnp.sum(jnp.where(eye, row, 0.0), axis=1, keepdims=True)


def spread_index(shape, j):
    lane = lax.broadcasted_iota(jnp.int32, shape, 1)
    return jnp.where(lane >= HEAD, 2 * j + 1, 2 * j)


def take_lanes(x, index):
    return jnp.take_along_axis(x, index, axis=1)


def spread_matrix(tile):
    row = lax.broadcasted_iota(jnp.int32, (LANES, 2 * LANES), 0)
    lane = lax.broadcasted_iota(jnp.int32, (LANES, 2 * LANES), 1)
    return jnp.where(row - lane // HEAD == 2 * LANES // HEAD * tile, 1.0, 0.0).astype(BF16)


def swap_matrix(outer, inner):
    size = outer * inner
    to = lax.broadcasted_iota(jnp.int32, (size, size), 0)
    source = lax.broadcasted_iota(jnp.int32, (size, size), 1)
    same = (to // inner == source % outer) & (to % inner == source // outer)
    return jnp.where(same, 1.0, 0.0).astype(BF16)


def lanes_to_rows(x):
    low = lax.broadcasted_iota(jnp.int32, (x.shape[0], LANES), 1) < HEAD
    out = []
    for c in range(0, x.shape[1], LANES):
        chunk = x[:, c : c + LANES]
        turned = pltpu.roll(chunk, HEAD, 1)
        out += [jnp.where(low, chunk, turned), jnp.where(low, turned, chunk)]
    return jnp.concatenate(out, axis=0)


def head_sums(x, rows, heads):
    sums = 0.5 * jnp.sum(x, axis=1, keepdims=True)
    lane = lax.broadcasted_iota(jnp.int32, (rows, heads), 1)
    out = jnp.zeros((rows, heads), F32)
    for h in range(heads):
        out = jnp.where(lane == h, sums[h * rows : (h + 1) * rows], out)
    return out


def readout_kernel(n_dp, width, heads, model, layer, *refs):
    parts, refs = refs[:n_dp], refs[n_dp:]
    bias, old_max, old_norm, memory, refs = *refs[:4], refs[4:]
    mixed_out, keep_out, admit_out, key_out, key_rows, value_rows, max_out = refs
    rows = mixed_out.shape[0]
    half = half_width(heads)
    total = tree_sum(p[...].astype(F32) for p in parts)
    tail = total[:, 4 * width :]
    tail = tail + pltpu.roll(tail, half, 1)
    inv = lax.rsqrt(tail[:, 2 * heads : 2 * heads + 1] / model + EPS)
    stored = [
        (inv * total[:, i * width : (i + 1) * width]).astype(BF16).astype(F32) for i in range(4)
    ]
    key = stored[1]
    turned = [lanes_to_rows(x) for x in stored]
    by_head = jnp.concatenate(turned, axis=1).astype(BF16)
    by_row = jnp.dot(swap_matrix(rows, heads), by_head, preferred_element_type=F32)
    query_rows = by_row[:, 0:LANES].astype(BF16)
    key_rows[...] = by_row[:, LANES : 2 * LANES].astype(BF16)
    value_row = by_row[:, 2 * LANES : 3 * LANES]
    value_rows[...] = value_row
    past = jnp.zeros((rows * heads, LANES), F32)
    for tile in range(HEAD * HEAD // (2 * LANES)):
        spread = jnp.dot(query_rows, spread_matrix(tile), preferred_element_type=F32)
        for c in range(0, 2 * LANES, LANES):
            at = tile * 2 * LANES + c
            block = memory[:, :, at : at + LANES].reshape(rows * heads, LANES)
            past = past + spread[:, c : c + LANES] * block
    past = past + pltpu.roll(past, HEAD, 1)

    input_pre = inv * tail[:, 0:heads]
    forget_pre = inv * tail[:, heads : 2 * heads] + bias[layer : layer + 1, :]
    log_forget = jnp.minimum(forget_pre, 0.0) - jnp.log1p(jnp.exp(-jnp.abs(forget_pre)))
    aged = log_forget + old_max[...]
    new_max = jnp.maximum(aged, input_pre)
    keep = jnp.exp(aged - new_max)
    admit = jnp.exp(input_pre - new_max) * HEAD**-0.5
    query_key = head_sums(turned[0] * turned[1], rows, heads)
    query_norm = head_sums(turned[0] * lanes_to_rows(old_norm[...]), rows, heads)
    gained = admit * query_key
    denominator = jnp.maximum(jnp.abs(keep * query_norm + gained), jnp.exp(-new_max))
    max_out[...] = new_max
    keep_out[...] = jnp.zeros_like(keep_out)
    admit_out[...] = jnp.zeros_like(admit_out)
    keep_out[:, 0:heads] = keep
    admit_out[:, 0:heads] = admit
    key_out[...] = key

    eye = lax.broadcasted_iota(jnp.int32, (heads, heads), 0) == lax.broadcasted_iota(
        jnp.int32, (heads, heads), 1
    )
    read = []
    for s in range(rows):
        at = slice(s * heads, (s + 1) * heads)
        numerator = (
            column(keep[s : s + 1], eye) * past[at] + column(gained[s : s + 1], eye) * value_row[at]
        )
        read.append(numerator / column(denominator[s : s + 1], eye))
    gate = by_row[:, 3 * LANES :]
    gated = (jnp.concatenate(read, axis=0) * jax.nn.sigmoid(gate)).astype(BF16)
    back = jnp.dot(swap_matrix(heads, rows), gated, preferred_element_type=F32)
    low = lax.broadcasted_iota(jnp.int32, (rows, LANES), 1) < HEAD
    for h in range(0, heads, 2):
        even, odd = back[h * rows : (h + 1) * rows], back[(h + 1) * rows : (h + 2) * rows]
        mixed_out[:, h * HEAD : (h + 2) * HEAD] = jnp.where(low, even, odd).astype(BF16)


def readout(parts, bias, old_max, old_norm, memory, layer, model):
    rows, heads = old_max.shape
    width = heads * HEAD
    out_shape = [
        jax.ShapeDtypeStruct((rows, width), BF16),
        jax.ShapeDtypeStruct((rows, LANES), F32),
        jax.ShapeDtypeStruct((rows, LANES), F32),
        jax.ShapeDtypeStruct((rows, width), F32),
        jax.ShapeDtypeStruct((rows * heads, LANES), BF16),
        jax.ShapeDtypeStruct((rows * heads, LANES), F32),
        jax.ShapeDtypeStruct((rows, heads), F32),
    ]
    in_specs = [VMEM] * (len(parts) + 4)
    return call(
        functools.partial(readout_kernel, len(parts), width, heads, model, layer),
        out_shape, in_specs, [VMEM] * len(out_shape), [], 20_000_000,
    )(*parts, bias, old_max, old_norm, memory)


def update_kernel(layer, *refs):
    keep_in, admit_in, key_in, key_rows, value_rows, max_in, memory, old_norm = refs[:8]
    refs = refs[8 + (3 if layer else 0) :]
    memory_out, norm_out, max_out, stage, norm, keep_rows, gain_rows, sems = refs
    rows, heads, size = memory.shape
    eye = lax.broadcasted_iota(jnp.int32, (heads, heads), 0) == lax.broadcasted_iota(
        jnp.int32, (heads, heads), 1
    )
    copies = [pltpu.make_async_copy(max_in, max_out.at[layer], sems.at[0])]
    copies[0].start()
    for j in range(heads * HEAD // LANES):
        cols = slice(j * LANES, (j + 1) * LANES)
        index = spread_index((rows, LANES), j)
        norm[:, cols] = (
            take_lanes(keep_in[...], index) * old_norm[:, cols]
            + take_lanes(admit_in[...], index) * key_in[:, cols]
        )
    copies.append(pltpu.make_async_copy(norm, norm_out.at[layer], sems.at[1]))
    copies[1].start()
    for s in range(rows):
        at = slice(s * heads, (s + 1) * heads)
        keep_rows[at] = jnp.broadcast_to(column(keep_in[s : s + 1, 0:heads], eye), (heads, LANES))
        gain_rows[at] = column(admit_in[s : s + 1, 0:heads], eye) * value_rows[at]
    tiles = size // (2 * LANES)
    group = tiles // (sems.shape[0] - 2)
    for tile in range(tiles):
        spread = jnp.dot(key_rows[...], spread_matrix(tile), preferred_element_type=F32)
        for c in range(0, 2 * LANES, LANES):
            cols = slice(tile * 2 * LANES + c, tile * 2 * LANES + c + LANES)
            block = memory[:, :, cols].reshape(rows * heads, LANES)
            fresh = keep_rows[...] * block + spread[:, c : c + LANES] * gain_rows[...]
            stage[:, :, cols] = fresh.reshape(rows, heads, LANES)
        if tile % group == group - 1:
            cols = pl.ds((tile - group + 1) * 2 * LANES, group * 2 * LANES)
            copies.append(
                pltpu.make_async_copy(
                    stage.at[:, :, cols], memory_out.at[layer, :, :, cols], sems.at[len(copies)]
                )
            )
            copies[-1].start()
    for copy in copies:
        copy.wait()


def update(read, memory, old_norm, layer, layers, earlier):
    rows, heads, size = memory.shape
    out_shape = [
        jax.ShapeDtypeStruct((layers, rows, heads, size), F32),
        jax.ShapeDtypeStruct((layers, rows, heads * HEAD), F32),
        jax.ShapeDtypeStruct((layers, rows, heads), F32),
    ]
    _, keep, admit, key, key_rows, value_rows, new_max = read
    in_specs = [VMEM] * 8 + ([HBM] * 3 if layer else [])
    return call(
        functools.partial(update_kernel, layer),
        out_shape, in_specs, [HBM] * 3,
        [
            pltpu.VMEM((rows, heads, size), F32),
            pltpu.VMEM((rows, heads * HEAD), F32),
            pltpu.VMEM((rows * heads, LANES), F32),
            pltpu.VMEM((rows * heads, LANES), F32),
            pltpu.SemaphoreType.DMA((2 + 4,)),
        ],
        20_000_000, {8: 0, 9: 1, 10: 2} if layer else None,
    )(keep, admit, key, key_rows, value_rows, new_max, memory, old_norm, *(earlier or ()))


def in_places(parts):
    n = len(parts)
    order = range(n) if is_pow2(n) else [-s % n for s in range(n)]
    return jnp.concatenate([parts[s][...].astype(F32) for s in order], axis=0).astype(BF16)


def out_kernel(n_dp, *refs):
    parts, weight, out = refs[:n_dp], refs[n_dp], refs[n_dp + 1]
    mixed = in_places(parts)
    step = min(weight.shape[1], 256)
    for c in range(0, weight.shape[1], step):
        out[:, c : c + step] = jnp.dot(
            mixed, weight[:, c : c + step], preferred_element_type=F32
        ).astype(BF16)


def last_out_kernel(n_dp, n_tp, *refs):
    parts, weight, refs = refs[:n_dp], refs[n_dp], refs[n_dp + 1 :]
    own, sends, acc = refs[0], refs[1:n_tp], refs[-1]
    me_tp, me_dp = lax.axis_index("tp"), lax.axis_index("dp")
    mixed = in_places(parts)
    step = min(weight.shape[1], 256)
    for c in range(0, weight.shape[1], step):
        acc[:, c : c + step] = jnp.dot(mixed, weight[:, c : c + step], preferred_element_type=F32)
    count = own.shape[0]

    def block(to):
        place = place_of(to, me_dp, n_dp)
        return acc[pl.ds(pl.multiple_of(place * count, count), count), :]

    own[...] = block(me_tp)
    for s in range(1, n_tp):
        sends[s - 1][...] = block(peer_to(me_tp, s, n_tp)).astype(BF16)


def out_projection(parts, weight, n_tp, last):
    n_dp = len(parts)
    rows, _ = parts[0].shape
    batch, columns = rows * n_dp, weight.shape[-1]
    in_specs = [VMEM] * (n_dp + 1)
    scratch = []
    if last:
        count = batch // n_tp
        out_shape = [jax.ShapeDtypeStruct((count, columns), F32)]
        out_shape += [jax.ShapeDtypeStruct((count, columns), BF16)] * (n_tp - 1)
        body = functools.partial(last_out_kernel, n_dp, n_tp)
        scratch.append(pltpu.VMEM((batch, columns), F32))
    else:
        out_shape = [jax.ShapeDtypeStruct((batch, columns), BF16)]
        body = functools.partial(out_kernel, n_dp)
    return call(
        body, out_shape, in_specs, [VMEM] * len(out_shape), scratch, 15_000_000
    )(*parts, weight)


def final_add(x, parts):
    return (x + tree_sum(p.astype(F32) for p in parts)).astype(BF16)


def plain_cell(parts, bias, old_max, old_norm, memory, layer, model):
    rows, heads = old_max.shape
    width, half = heads * HEAD, half_width(heads)
    total = tree_sum(p.astype(F32) for p in parts)
    tail = total[:, 4 * width : 4 * width + half] + total[:, 4 * width + half :]
    inv = lax.rsqrt(tail[:, 2 * heads : 2 * heads + 1] / model + EPS)
    stored = lax.optimization_barrier((inv * total[:, : 4 * width]).astype(BF16)).astype(F32)
    query, key, value, gate = (
        stored[:, i * width : (i + 1) * width].reshape(rows, heads, HEAD) for i in range(4)
    )
    key = key * HEAD**-0.5
    input_pre = inv * tail[:, 0:heads]
    forget_pre = inv * tail[:, heads : 2 * heads] + bias[layer][None, :]
    aged = jax.nn.log_sigmoid(forget_pre) + old_max
    new_max = jnp.maximum(aged, input_pre)
    keep, admit = jnp.exp(aged - new_max), jnp.exp(input_pre - new_max)
    state = memory.reshape(rows, heads, HEAD, HEAD)
    state = (
        keep[:, :, None, None] * state
        + admit[:, :, None, None] * key[:, :, :, None] * value[:, :, None, :]
    )
    norm = keep[:, :, None] * old_norm.reshape(rows, heads, HEAD) + admit[:, :, None] * key
    top = jnp.einsum("bhd,bhde->bhe", query, state, precision=lax.Precision.HIGHEST)
    bottom = jnp.maximum(jnp.abs(jnp.sum(query * norm, axis=2)), jnp.exp(-new_max))
    mixed = (top / bottom[:, :, None] * jax.nn.sigmoid(gate)).astype(BF16).reshape(rows, width)
    return mixed, state.reshape(rows, heads, -1), norm.reshape(rows, width), new_max


def fills_tiles(memory):
    return memory.shape[1] % 8 == 0 and memory.shape[2] % 8 == 0


def per_device(
    n_tp, n_dp, tokens, norm_gain, query_weight, key_weight, value_weight, outgate_weight,
    input_gate_weight, forget_gate_weight, forget_bias, out_weight, memory_state,
    normalizer_state, maximum_state,
):
    layers = memory_state.shape[0]
    batch = tokens.shape[0] * n_tp
    model = query_weight.shape[1] * n_dp
    weights = (query_weight, key_weight, value_weight, outgate_weight)
    gates = tuple(jnp.swapaxes(g, 1, 2) for g in (input_gate_weight, forget_gate_weight))
    x_all = None
    pieces = exchange([tokens] * (n_tp - 1), "tp", n_tp)
    own, gain, *used = load((tokens, norm_gain), (*gates, *weights), 0)
    pieces = [own] + pieces
    tiled = fills_tiles(memory_state)
    assert n_tp == n_dp and batch == n_dp * memory_state.shape[1]
    states, plain = None, []
    for layer in range(layers):
        last = layer == layers - 1
        x_all, own, sends = projection(
            x_all, pieces, layer, last, gain, used[2:], used[:2], batch, n_tp, n_dp
        )
        parts = [own] + exchange(sends, "dp", n_dp)
        bias, old_max, old_norm, memory, project_out = load(
            (forget_bias,), (maximum_state, normalizer_state, memory_state, out_weight),
            layer,
        )
        if tiled:
            read = readout(parts, bias, old_max, old_norm, memory, layer, model)
            mixed = read[0]
        else:
            mixed, *rest = plain_cell(parts, bias, old_max, old_norm, memory, layer, model)
            plain.append(rest)
        mixes = [mixed] + exchange([mixed] * (n_dp - 1), "dp", n_dp)
        if tiled:
            states = update(read, memory, old_norm, layer, layers, states)
        part = out_projection(mixes, project_out, n_tp, last)
        sends = part[1:] if last else [part[0]] * (n_tp - 1)
        pieces = [part[0]] + exchange(sends, "tp", n_tp)
        if not last:
            used = load((), (*gates, *weights), layer + 1)
    next_tokens = final_add(x_all, pieces)
    if plain:
        states = [jnp.stack(column) for column in zip(*plain)]
    return (next_tokens, *states)


def solution(mesh):
    sizes = dict(mesh.shape)
    in_specs = (
        P(("grp", "tp"), "dp"),
        P(None, "dp"),
        P(None, "dp", "tp"),
        P(None, "dp", "tp"),
        P(None, "dp", "tp"),
        P(None, "dp", "tp"),
        P(None, "dp", "tp"),
        P(None, "dp", "tp"),
        P(None, "tp"),
        P(None, "tp", "dp"),
        P(None, ("grp", "dp"), "tp", None),
        P(None, ("grp", "dp"), "tp"),
        P(None, ("grp", "dp"), "tp"),
    )
    out_specs = (
        P(("grp", "tp"), "dp"),
        P(None, ("grp", "dp"), "tp", None),
        P(None, ("grp", "dp"), "tp"),
        P(None, ("grp", "dp"), "tp"),
    )
    n_tp, n_dp = sizes["tp"], sizes["dp"]

    def whole(*args):
        return per_device(n_tp, n_dp, *args)

    def step(*args):
        sharded = jax.shard_map(
            whole, mesh=mesh, in_specs=in_specs, out_specs=out_specs, check_vma=False
        )
        return sharded(*args)

    return step
```
